256 devices in a mesh: grp: 2 (over y), fs: 16 (over z), tp: 8 (over x, core).
Axes of the slice: x: 4, y: 2, z: 16, core: 2. Of those that a mesh axis runs over, the one named last changes fastest.
The devices are a block of a 4x16x16 slice.
Arguments:
- tokens: bfloat16 [32768, 2048], P(('grp', 'fs', 'tp')), parts along dimension 0, may hold values from -6 to 6
- norm_gains: float32 [4, 2048], replicated, may hold values from 0.1 to 1.9
- query_weight: bfloat16 [2048, 2048], P('fs', 'tp'), may hold values from -0.125 to 0.125
- key_weight: bfloat16 [2048, 2048], P('fs', 'tp'), may hold values from -0.125 to 0.125
- value_weight: bfloat16 [2048, 4096], P('fs', 'tp'), may hold values from -0.125 to 0.125
- swish_weight: bfloat16 [2048, 4096], P('fs', 'tp'), may hold values from -0.125 to 0.125
- mixer_output: bfloat16 [4096, 2048], P('tp', 'fs'), may hold values from -0.09375 to 0.09375
- gate_weight: bfloat16 [2048, 3072], P('fs', 'tp'), may hold values from -0.125 to 0.125
- up_weight: bfloat16 [2048, 3072], P('fs', 'tp'), may hold values from -0.125 to 0.125
- down_weight: bfloat16 [3072, 2048], P('tp', 'fs'), may hold values from -0.109375 to 0.109375
Outputs:
- layer_output: bfloat16 [32768, 2048], P(('grp', 'fs', 'tp')), parts along dimension 0
The draws below stay inside these ranges and needn't reach their ends.
There are 2 independent parts, one for each index of `grp`. The reference program is written for one: setup_inputs(seed, part) draws one part's arguments, and reference() takes and returns one part's arrays. A program takes and returns all parts, laid end to end along the dimension named above; an argument that names none is the same for every part. Nothing has to cross between parts.
All inputs are finite; a program needn't handle non-finite values.
Results may differ from the reference program's by a relative error of at most 0.02.
Values may be sent and summed in bfloat16 or wider, within the bound.
A program may use at most 64 MiB of HBM per device.

```python
import jax
import jax.numpy as jnp
from jax import lax

D = 2048
H = 8
QK = 256
VD = 512
FF = 3072
BLOCK = 128
SEQ = 1024
TOKENS = 16384
N_TP = 8


def levels(own_key, shape, pieces, low, top_value):
    level, own = 1.0, jax.random.fold_in(own_key, 6)
    for dim, parts in pieces:
        draws = jnp.exp(jax.random.uniform(jax.random.fold_in(own, dim), (parts,), jnp.float32, low / len(pieces), top_value / len(pieces)))
        level = level * jnp.repeat(draws, shape[dim] // parts).reshape([-1 if axis == dim else 1 for axis in range(len(shape))])
    return level


def noise(key, extent, deviation, most, split=(), kind=jnp.bfloat16):
    level = levels(key, extent, split, -0.22, 0.18) if split else 1.0
    array = jax.random.normal(key, extent, jnp.float32) * deviation * level
    return jnp.minimum(jnp.maximum(array, -most), most).astype(kind)


def setup_inputs(seed: int = 0, part: int = 0) -> dict:
    key_of = jax.random.split(jax.random.key(seed), 11)
    part_splits = jax.random.split(jax.random.fold_in(key_of[10], part), 11)
    tokens = noise(part_splits[0], (TOKENS, D), 1.0, 6.0, ((0, 128),))
    norm_gains = jnp.clip(1.0 + 0.18 * jax.random.normal(key_of[1], (4, D), jnp.float32), 0.1, 1.9)
    query_weight = noise(key_of[2], (D, H * QK), D ** -0.5, 0.125, ((0, 16), (1, 8)))
    key_weight = noise(key_of[3], (D, H * QK), D ** -0.5, 0.125, ((0, 16), (1, 8)))
    value_weight = noise(key_of[4], (D, H * VD), D ** -0.5, 0.125, ((0, 16), (1, 8)))
    swish_weight = noise(key_of[5], (D, H * VD), D ** -0.5, 0.125, ((0, 16), (1, 8)))
    mixer_output = noise(key_of[6], (H * VD, D), (H * VD) ** -0.5, 0.09375, ((0, 8), (1, 16)))
    gate_weight = noise(key_of[7], (D, FF), D ** -0.5, 0.125, ((0, 16), (1, 8)))
    up_weight = noise(key_of[8], (D, FF), D ** -0.5, 0.125, ((0, 16), (1, 8)))
    down_weight = noise(key_of[9], (FF, D), FF ** -0.5, 0.109375, ((0, 8), (1, 16)))
    return dict(tokens=tokens, norm_gains=norm_gains, query_weight=query_weight, key_weight=key_weight, value_weight=value_weight, swish_weight=swish_weight, mixer_output=mixer_output, gate_weight=gate_weight, up_weight=up_weight, down_weight=down_weight)


norm_epsilon = 1e-06
group_epsilon = 0.01

def rms_scale(matrix, gain):
    return matrix * lax.rsqrt(lax.optimization_barrier(jnp.mean(matrix * matrix, axis=-1, keepdims=True)) + norm_epsilon) * gain

def rotate_halves(head_tensors, cosine_table, sine_table):
    half_width = head_tensors.shape[-1] // 2
    lower_half = head_tensors[..., :half_width]
    upper_half = head_tensors[..., half_width:]
    return jnp.concatenate([lower_half * cosine_table - upper_half * sine_table, lower_half * sine_table + upper_half * cosine_table], axis=-1)

def decayed_sum(queries, key_rows, value_rows, log_decay):
    query_expanded = queries.astype(jnp.float32)
    key_expanded = key_rows.astype(jnp.float32)
    value_wide = value_rows.astype(jnp.float32)
    retention_scores = jnp.einsum('fzy,czy->zfc', query_expanded, key_expanded)
    offsets = jnp.arange(queries.shape[0], dtype=jnp.float32)
    distance = offsets[:, None] - offsets[None, :]
    weights = jnp.where(distance >= 0, jnp.exp(log_decay[:, None, None] * jnp.maximum(distance, 0.0)), 0.0)
    return jnp.einsum('hnm,mhe->nhe', retention_scores * weights, value_wide)

def grouped_product(active, weight):
    group_width = active.shape[1] // N_TP
    running = jnp.zeros((active.shape[0], weight.shape[1]), jnp.float32)
    for group_index in range(N_TP):
        lower = group_index * group_width
        product = jnp.dot(active[:, lower:lower + group_width], weight[lower:lower + group_width], preferred_element_type=jnp.float32)
        rounded = lax.optimization_barrier(product.astype(jnp.bfloat16))
        running = running + rounded.astype(jnp.float32)
    return running

def reference(tokens, norm_gains, query_weight, key_weight, value_weight, swish_weight, mixer_output, gate_weight, up_weight, down_weight):
    residual = tokens.astype(jnp.float32)
    normed = rms_scale(residual, norm_gains[0]).astype(jnp.bfloat16)
    raw_query = jnp.dot(normed, query_weight, preferred_element_type=jnp.float32)
    raw_keys = jnp.dot(normed, key_weight, preferred_element_type=jnp.float32)
    raw_values = jnp.dot(normed, value_weight, preferred_element_type=jnp.float32)
    raw_swish = jnp.dot(normed, swish_weight, preferred_element_type=jnp.float32)
    seq_count = tokens.shape[0] // SEQ
    positions = jnp.arange(SEQ, dtype=jnp.float32)
    frequency = 10000.0 ** (-jnp.linspace(0.0, 1.0, QK // 2, dtype=jnp.float32))
    angles = positions[:, None] * frequency[None, :]
    cosine_table = jnp.cos(angles)[:, None, :]
    sine_table = jnp.sin(angles)[:, None, :]
    queries = rotate_halves(raw_query.reshape(seq_count, SEQ, H, QK), cosine_table, sine_table).astype(jnp.bfloat16)
    key_rows = (rotate_halves(raw_keys.reshape(seq_count, SEQ, H, QK), cosine_table, sine_table) * QK ** (-0.5)).astype(jnp.bfloat16)
    value_rows = raw_values.reshape(seq_count, SEQ, H, VD).astype(jnp.bfloat16)
    head_index = jnp.arange(H, dtype=jnp.float32)
    log_decay = -(4.0 / BLOCK) * (BLOCK / (32.0 * SEQ)) ** (head_index / (H - 1))
    retained = lax.map(lambda triple: decayed_sum(triple[0], triple[1], triple[2], log_decay), (queries, key_rows, value_rows))
    centred = retained - lax.optimization_barrier(jnp.mean(retained, axis=-1, keepdims=True))
    normalized = centred * lax.rsqrt(lax.optimization_barrier(jnp.mean(centred * centred, axis=-1, keepdims=True)) + group_epsilon)
    gated_rows = (jax.nn.silu(raw_swish) * normalized.reshape(tokens.shape[0], H * VD)).astype(jnp.bfloat16)
    mixer_total = grouped_product(gated_rows, mixer_output)
    after_mixer = residual + rms_scale(mixer_total, norm_gains[1])
    widened = rms_scale(after_mixer, norm_gains[2]).astype(jnp.bfloat16)
    gate_sum = jnp.dot(widened, gate_weight, preferred_element_type=jnp.float32)
    up_sum = jnp.dot(widened, up_weight, preferred_element_type=jnp.float32)
    hidden = (jax.nn.silu(gate_sum) * up_sum).astype(jnp.bfloat16)
    channel = grouped_product(hidden, down_weight)
    return (after_mixer + rms_scale(channel, norm_gains[3])).astype(jnp.bfloat16)
```

```python
import functools

import jax
import jax.numpy as jnp
import numpy as np
from jax import lax
from jax.experimental import pallas as pl
from jax.experimental.pallas import tpu as pltpu
from jax.sharding import PartitionSpec as P

H = 8
BLOCK = 128
norm_epsilon = 1e-06
group_epsilon = 0.01
MESH = pl.DeviceIdType.MESH
F32 = jnp.float32
BF16 = jnp.bfloat16


def mod(a, n):
    return lax.rem(a + n, n)


def rms(matrix):
    return matrix * lax.rsqrt(jnp.mean(matrix * matrix, axis=-1, keepdims=True) + norm_epsilon)


def silu(v):
    return v / (1.0 + jnp.exp(-v))


def kernel(
    nf,
    nx,
    tok,
    gains,
    lam_ref,
    cos_hbm,
    sin_hbm,
    wq,
    wk,
    wv,
    ws,
    wo,
    wg,
    wu,
    wd,
    out,
    w1,
    w2,
    w3,
    w4,
    xn,
    xw,
    acc,
    qb,
    kb,
    vb,
    gp,
    hid,
    part,
    sib_in,
    stage,
    pass_in,
    from_left,
    from_right,
    am,
    cos,
    sin,
    decay,
    local_sem,
    z_send,
    z_recv,
    y_send,
    y_recv,
    g_send,
    g_recv,
    s_send,
    s_recv,
    r_send,
    r_recv,
):
    rows, width = tok.shape
    seq = xn.shape[0]
    half = width // 2
    quarter = seq // 4
    me = lax.axis_index("fs")
    tp = lax.axis_index("tp")
    group = lax.axis_index("grp")
    x = tp // 2
    core = lax.rem(tp, 2)
    plane = lax.rem(group, 2)
    up = {"fs": mod(me + 1, nf)}
    down = {"fs": mod(me - 1, nf)}
    pair = {"grp": group + 1 - 2 * plane}
    sib = {"tp": 2 * x + 1 - core}
    right = {"tp": 2 * mod(x + 1, nx) + core}
    left = {"tp": 2 * mod(x - 1, nx) + core}

    def copy(src, dst, send, recv, device):
        return pltpu.make_async_remote_copy(
            src_ref=src,
            dst_ref=dst,
            send_sem=send,
            recv_sem=recv,
            device_id=device,
            device_id_type=MESH,
        )

    kd = wq.shape[0]
    mine = pl.ds(pl.multiple_of(me * kd, kd), kd)
    mine_cols = pl.ds(pl.multiple_of(me * kd, kd), kd)
    qw, vw, ff = wq.shape[1], wv.shape[1], wg.shape[1]
    locals_ = [
        (wq, w1.at[mine, 0:qw]),
        (wk, w1.at[mine, qw : 2 * qw]),
        (wv, w1.at[mine, 2 * qw : 2 * qw + vw]),
        (ws, w1.at[mine, 2 * qw + vw : 2 * qw + 2 * vw]),
        (wo, w2.at[:, mine_cols]),
        (wg, w3.at[mine, 0:ff]),
        (wu, w3.at[mine, ff : 2 * ff]),
        (wd, w4.at[:, mine_cols]),
        (cos_hbm, cos),
        (sin_hbm, sin),
    ]
    loads = [
        pltpu.make_async_copy(src, dst, local_sem.at[i]) for i, (src, dst) in enumerate(locals_)
    ]
    for load in loads:
        load.start()

    barrier = pltpu.get_barrier_semaphore()
    for device in (up, down, pair, sib, right, left):
        pl.semaphore_signal(barrier, inc=1, device_id=device, device_id_type=MESH)

    own = pl.multiple_of(tp * rows, rows)

    def norm_in(i, carry):
        at = pl.multiple_of(i * 16, 16)
        value = rms(tok[pl.ds(at, 16), :].astype(F32)) * gains[0:1, :]
        xn[pl.ds(own + at, 16), :] = value.astype(BF16)
        return carry

    lax.fori_loop(0, rows // 16, norm_in, 0)
    pl.semaphore_wait(barrier, 6)

    def third(total):
        return total // 3 // 16 * 16 + (16 if total // 3 % 16 else 0)

    def place(a, owner, piece, plane_, rows_half=None):
        ref = (w1, w2, w3, w4)[a]
        if a in (0, 2):
            w = ref.shape[1] // 3
            start, count = owner * kd, kd
            if rows_half is not None:
                count = kd // 2
                start = start + rows_half * count
            r = pl.ds(pl.multiple_of(start, kd // 2), count)
            c = pl.ds(pl.multiple_of(plane_ * 2 * w, 128), w) if piece == 0 else pl.ds(w, w)
            return ref.at[r, c]
        t = third(ref.shape[0])
        mid = ref.shape[0] - 2 * t
        r = pl.ds(pl.multiple_of(plane_ * (t + mid), 16), t) if piece == 0 else pl.ds(t, mid)
        return ref.at[r, pl.ds(pl.multiple_of(owner * kd, kd), kd)]

    def owner_of(d, s):
        return mod(me - s, nf) if d == 0 else lax.rem(me + s, nf)

    far = nf // 2

    def z_copy(a, d, piece, s, rows_half=None):
        src = place(a, owner_of(d, s - 1), piece, plane, rows_half)
        k = (a * 2 + d) * 2 + piece
        return copy(src, src, z_send.at[k], z_recv.at[k, s - 1], up if d == 0 else down)

    def z_arrived(a, d, piece, s, rows_half=None):
        dst = place(a, owner_of(d, s), piece, plane, rows_half)
        k = (a * 2 + d) * 2 + piece
        copy(dst, dst, z_send.at[k], z_recv.at[k, s - 1], up if d == 0 else down).wait_recv()

    def y_copy(a, d, s, rows_half=None):
        src = place(a, owner_of(d, s), 0, plane, rows_half)
        k = a * 2 + d
        return copy(src, src, y_send.at[k], y_recv.at[k, s - 1], pair)

    def y_arrived(a, d, s, rows_half=None):
        dst = place(a, owner_of(d, s), 0, 1 - plane, rows_half)
        k = a * 2 + d
        copy(dst, dst, y_send.at[k], y_recv.at[k, s - 1], pair).wait_recv()

    def last_half(a, d):
        return d if a in (0, 2) else None

    def has_last(a, d):
        return a in (0, 2) or (a == 1 and d == 0) or (a == 3 and d == 1)

    def pump_start(arrays):
        for piece in (0, 1):
            for a in arrays:
                for d in (0, 1):
                    z_copy(a, d, piece, 1).start()

    def pump(arrays, s, first=False):
        for piece in (0, 1):
            for a in arrays:
                for d in (0, 1):
                    z_arrived(a, d, piece, s)
                    z_copy(a, d, piece, s).wait_send()
                    z_copy(a, d, piece, s + 1).start()
                    if piece == 0:
                        if not first:
                            y_copy(a, d, s - 1).wait_send()
                        y_copy(a, d, s).start()

    def pump_before_last(arrays):
        s = far - 1
        for piece in (0, 1):
            for a in arrays:
                for d in (0, 1):
                    z_arrived(a, d, piece, s)
                    z_copy(a, d, piece, s).wait_send()
                    if has_last(a, d):
                        z_copy(a, d, piece, s + 1, last_half(a, d)).start()
                    if piece == 0:
                        y_copy(a, d, s - 1).wait_send()
                        y_copy(a, d, s).start()

    def pump_last(arrays):
        for piece in (0, 1):
            for a in arrays:
                for d in (0, 1):
                    if has_last(a, d):
                        z_arrived(a, d, piece, far, last_half(a, d))
                        z_copy(a, d, piece, far, last_half(a, d)).wait_send()
                    if piece == 0:
                        y_copy(a, d, far - 1).wait_send()
                        if has_last(a, d):
                            y_copy(a, d, far, last_half(a, d)).start()

    def y_all(a, s):
        for d in (0, 1):
            if s is far:
                if has_last(a, d):
                    y_arrived(a, d, far, last_half(a, d))
            else:
                y_arrived(a, d, s)

    def y_drain(a):
        for d in (0, 1):
            if has_last(a, d):
                y_copy(a, d, far, last_half(a, d)).wait_send()

    def gather(n, ref, block):
        at_left, at_right, at_far = mod(x - 1, nx), mod(x + 1, nx), mod(x + 2, nx)
        lo, hi = pl.ds(0, half), pl.ds(half, half)
        every = pl.ds(0, width)

        def whole(xx, cc, cols=every):
            return ref.at[pl.ds(pl.multiple_of(block(xx, cc) * rows, rows), rows), cols]

        def send(k, xx, cols, device):
            src = whole(xx, core, cols)
            return copy(src, src, g_send.at[n, k], g_recv.at[n, k], device)

        def arrived(k, xx, cc, cols):
            dst = whole(xx, cc, cols)
            copy(dst, dst, g_send.at[n, k], g_recv.at[n, k], sib).wait_recv()

        sends = []

        def go(*args):
            s = send(*args)
            s.start()
            sends.append(s)

        def first():
            go(1, x, every, right)
            go(2, x, every, left)
            go(0, x, every, sib)

        def second():
            arrived(1, at_left, core, every)
            go(3, at_left, lo, right)
            go(4, at_left, every, sib)
            arrived(2, at_right, core, every)
            go(5, at_right, hi, left)
            go(6, at_right, every, sib)

        def third_():
            arrived(3, at_far, core, lo)
            go(7, at_far, lo, sib)
            arrived(5, at_far, core, hi)
            go(8, at_far, hi, sib)

        def own_chip():
            arrived(0, x, 1 - core, every)

        def near():
            arrived(4, at_left, 1 - core, every)
            arrived(6, at_right, 1 - core, every)

        def rest():
            arrived(7, at_far, 1 - core, lo)
            arrived(8, at_far, 1 - core, hi)

        def drain():
            for s in sends:
                s.wait_send()

        return first, second, third_, own_chip, near, rest, drain

    for load in loads[:5]:
        load.wait()
    pump_start((0, 1))
    first, second, third_, own_chip, near, rest, drain1 = gather(0, xn, lambda xx, cc: 2 * xx + cc)
    first()

    lam = lam_ref[0:1, 0:1]
    dn = lax.broadcasted_iota(jnp.int32, decay.shape, 0) + (seq - quarter)
    dm = lax.broadcasted_iota(jnp.int32, decay.shape, 1)
    dist = (dn - dm).astype(F32)
    decay[...] = jnp.where(dist >= 0.0, jnp.exp(lam * jnp.maximum(dist, 0.0)), 0.0)
    for load in loads[5:]:
        load.wait()

    def k_slice(owner):
        return pl.ds(pl.multiple_of(owner * kd, kd), kd)

    def add_own():
        def body(i, carry):
            r = pl.ds(pl.multiple_of(i * quarter, quarter), quarter)
            acc[r, :] = jnp.dot(
                xn[r, k_slice(me)], w1[k_slice(me), :], preferred_element_type=F32
            )
            return carry

        lax.fori_loop(0, 4, body, 0)

    def add_two(s):
        a, b = k_slice(owner_of(0, s)), k_slice(owner_of(1, s))

        def body(i, carry):
            r = pl.ds(pl.multiple_of(i * quarter, quarter), quarter)
            acc[r, :] = (
                acc[r, :]
                + jnp.dot(xn[r, a], w1[a, :], preferred_element_type=F32)
                + jnp.dot(xn[r, b], w1[b, :], preferred_element_type=F32)
            )
            return carry

        lax.fori_loop(0, 4, body, 0)

    pump((0, 1), 1, first=True)
    second()
    pump((0, 1), 2)
    own_chip()
    third_()
    near()
    rest()
    add_own()
    y_all(0, 1)
    add_two(1)

    def steps(s, carry):
        pump((0, 1), s)
        y_all(0, s - 1)
        add_two(s - 1)
        return carry

    lax.fori_loop(3, far - 1, steps, 0)
    pump_before_last((0, 1))
    pump_start((2, 3))
    y_all(0, far - 2)
    add_two(far - 2)
    pump_last((0, 1))
    y_all(0, far - 1)
    add_two(far - 1)
    y_all(0, far)
    far_slice = k_slice(owner_of(0, far))

    key_scale = float(qw) ** -0.5
    hq = qw // 2

    def finish(i, carry):
        r = pl.ds(pl.multiple_of(i * quarter, quarter), quarter)
        total = acc[r, :] + jnp.dot(xn[r, far_slice], w1[far_slice, :], preferred_element_type=F32)
        c, s = cos[r, :], sin[r, :]
        for ref, at, scale in ((qb, 0, None), (kb, qw, key_scale)):
            a, b = total[:, at : at + hq], total[:, at + hq : at + qw]
            first_half = a * c - b * s
            second_half = a * s + b * c
            if scale is not None:
                first_half, second_half = first_half * scale, second_half * scale
            ref[r, 0:hq] = first_half.astype(BF16)
            ref[r, hq:qw] = second_half.astype(BF16)
        vb[r, :] = total[:, 2 * qw : 2 * qw + vw].astype(BF16)
        acc[r, 2 * qw + vw :] = total[:, 2 * qw + vw :]
        return carry

    lax.fori_loop(0, 4, finish, 0)
    pump((2, 3), 1, first=True)

    def retain(i):
        r = slice(i * quarter, (i + 1) * quarter)
        seen = (i + 1) * quarter
        scores = lax.dot_general(
            qb[r, :], kb[0:seen, :], (((1,), (1,)), ((), ())), preferred_element_type=F32
        )
        weighted = (scores * decay[:, seq - seen :]).astype(BF16)
        retained = jnp.dot(weighted, vb[0:seen, :], preferred_element_type=F32)
        centred = retained - jnp.mean(retained, axis=-1, keepdims=True)
        normalized = centred * lax.rsqrt(
            jnp.mean(centred * centred, axis=-1, keepdims=True) + group_epsilon
        )
        gated = (silu(acc[r, 2 * qw + vw :]) * normalized).astype(BF16)
        gp[i * rows : (i + 1) * rows, :] = gated[0:rows, :]
        gp[(nx + i) * rows : (nx + i + 1) * rows, :] = gated[rows:, :]

    retain(0)
    retain(1)
    pump((2, 3), 2)
    retain(2)
    retain(3)
    y_all(1, 1)
    for s in range(2, far):
        y_all(1, s)
    y_all(1, far)
    pump((2, 3), 3)

    def project(lhs, weight, cc):
        r = pl.ds(pl.multiple_of(cc * nx * rows, rows), nx * rows)
        n = width // 4

        def body(j, carry):
            cols = pl.ds(pl.multiple_of(j * n, n), n)
            part[r, cols] = jnp.dot(lhs[r, :], weight[:, cols], preferred_element_type=F32).astype(
                BF16
            )
            return carry

        lax.fori_loop(0, 4, body, 0)

    def reduce(n, lhs, weight, pumps):
        lo, hi = slice(0, half), slice(half, width)
        near_x = (mod(x + 2, nx), mod(x + 1, nx), mod(x - 1, nx), x)

        def rows_of(cc, xx):
            return pl.ds(pl.multiple_of((cc * nx + xx) * rows, rows), rows)

        project(lhs, weight, 1 - core)
        sends = []
        arrivals = []
        for k, xx in enumerate(near_x):
            s = copy(
                part.at[rows_of(1 - core, xx), :],
                sib_in.at[n, k],
                s_send.at[n, k],
                s_recv.at[n, k],
                sib,
            )
            s.start()
            sends.append(s)
            arrivals.append(s)
        project(lhs, weight, core)

        def pre(k, cols):
            return part[rows_of(core, near_x[k]), cols].astype(F32) + sib_in[n, k, :, cols].astype(
                F32
            )

        def ship(k, src, dst, device):
            s = copy(src, dst, r_send.at[n, k], r_recv.at[n, k], device)
            s.start()
            sends.append(s)
            arrivals.append(s)

        arrivals[0].wait_recv()
        stage[n, 0, :, hi] = pre(0, hi).astype(BF16)
        ship(0, stage.at[n, 0, :, hi], pass_in.at[n, 0], right)
        stage[n, 0, :, lo] = pre(0, lo).astype(BF16)
        ship(1, stage.at[n, 0, :, lo], pass_in.at[n, 1], left)
        arrivals[1].wait_recv()
        stage[n, 1, :, lo] = pre(1, lo).astype(BF16)
        ship(2, stage.at[n, 1, :, lo], from_left.at[n, :, lo], right)
        arrivals[2].wait_recv()
        stage[n, 2, :, hi] = pre(2, hi).astype(BF16)
        ship(3, stage.at[n, 2, :, hi], from_right.at[n, :, hi], left)
        pumps[0]()
        arrivals[4].wait_recv()
        stage[n, 1, :, hi] = (pre(1, hi) + pass_in[n, 0].astype(F32)).astype(BF16)
        ship(4, stage.at[n, 1, :, hi], from_left.at[n, :, hi], right)
        arrivals[5].wait_recv()
        stage[n, 2, :, lo] = (pre(2, lo) + pass_in[n, 1].astype(F32)).astype(BF16)
        ship(5, stage.at[n, 2, :, lo], from_right.at[n, :, lo], left)
        arrivals[3].wait_recv()
        pumps[1]()
        for k in (6, 7, 8, 9):
            arrivals[k].wait_recv()

        def total(at, count):
            r = pl.ds(at, count)
            here = part[pl.ds((core * nx + x) * rows + at, count), :].astype(F32)
            return (
                (here + sib_in[n, 3, r, :].astype(F32))
                + from_left[n, r, :].astype(F32)
                + from_right[n, r, :].astype(F32)
            )

        def drain():
            for s in sends:
                s.wait_send()

        return total, drain

    def pumps_a():
        pump((2, 3), 4)

    def pumps_b():
        pump((2, 3), 5)
        pump((2, 3), 6)

    total, drain2 = reduce(0, gp, w2, (pumps_a, pumps_b))
    wide_own = (core * nx + x) * rows

    def mixed(i, carry):
        at = pl.multiple_of(i * 16, 16)
        after = tok[pl.ds(at, 16), :].astype(F32) + rms(total(at, 16)) * gains[1:2, :]
        am[pl.ds(at, 16), :] = after
        xw[pl.ds(pl.multiple_of(wide_own + at, 16), 16), :] = (rms(after) * gains[2:3, :]).astype(
            BF16
        )
        return carry

    lax.fori_loop(0, rows // 16, mixed, 0)
    first, second, third_, own_chip, near, rest, drain3 = gather(1, xw, lambda xx, cc: cc * nx + xx)
    first()
    pump_before_last((2, 3))
    second()
    pump_last((2, 3))
    for a in (2, 3):
        for s in range(1, far):
            y_all(a, s)
        y_all(a, far)
    own_chip()
    third_()
    near()
    rest()
    drain2()

    def feed(i, carry):
        r = pl.ds(pl.multiple_of(i * quarter, quarter), quarter)
        both = jnp.dot(xw[r, :], w3[...], preferred_element_type=F32)
        hid[r, :] = (silu(both[:, 0:ff]) * both[:, ff:]).astype(BF16)
        return carry

    lax.fori_loop(0, 4, feed, 0)
    total, drain4 = reduce(1, hid, w4, (lambda: None, lambda: None))

    def last(i, carry):
        at = pl.multiple_of(i * 16, 16)
        r = pl.ds(at, 16)
        out[r, :] = (am[r, :] + rms(total(at, 16)) * gains[3:4, :]).astype(BF16)
        return carry

    lax.fori_loop(0, rows // 16, last, 0)
    drain1()
    drain3()
    drain4()
    for a in range(4):
        y_drain(a)


def layer(nf, nx, tokens, gains, wq, wk, wv, ws, wo, wg, wu, wd):
    rows, width = tokens.shape
    seq = rows * 2 * nx
    qw, vw, ff = wq.shape[1], wv.shape[1], wg.shape[1]
    frequency = 10000.0 ** (-np.linspace(0.0, 1.0, qw // 2))
    angles = np.arange(seq, dtype=np.float64)[:, None] * frequency[None, :]
    cos = jnp.asarray(np.cos(angles).astype(np.float32))
    sin = jnp.asarray(np.sin(angles).astype(np.float32))
    head = lax.axis_index("tp").astype(F32)
    lam = -(4.0 / BLOCK) * (BLOCK / (32.0 * seq)) ** (head / (H - 1))
    lam = jnp.full((8, 128), lam, F32)
    vmem = pl.BlockSpec(memory_space=pltpu.VMEM)
    hbm = pl.BlockSpec(memory_space=pl.ANY)
    dma = pltpu.SemaphoreType.DMA
    far = nf // 2
    half = width // 2
    n1 = 2 * qw + 2 * vw
    return pl.pallas_call(
        functools.partial(kernel, nf, nx),
        out_shape=jax.ShapeDtypeStruct((rows, width), BF16),
        in_specs=[vmem] * 3 + [hbm] * 10,
        out_specs=vmem,
        scratch_shapes=[
            pltpu.VMEM((width, n1), BF16),
            pltpu.VMEM((wo.shape[0], width), BF16),
            pltpu.VMEM((width, 2 * ff), BF16),
            pltpu.VMEM((wd.shape[0], width), BF16),
            pltpu.VMEM((seq, width), BF16),
            pltpu.VMEM((seq, width), BF16),
            pltpu.VMEM((seq, n1), F32),
            pltpu.VMEM((seq, qw), BF16),
            pltpu.VMEM((seq, qw), BF16),
            pltpu.VMEM((seq, vw), BF16),
            pltpu.VMEM((seq, vw), BF16),
            pltpu.VMEM((seq, ff), BF16),
            pltpu.VMEM((seq, width), BF16),
            pltpu.VMEM((2, nx, rows, width), BF16),
            pltpu.VMEM((2, 3, rows, width), BF16),
            pltpu.VMEM((2, 2, rows, half), BF16),
            pltpu.VMEM((2, rows, width), BF16),
            pltpu.VMEM((2, rows, width), BF16),
            pltpu.VMEM((rows, width), F32),
            pltpu.VMEM((seq, qw // 2), F32),
            pltpu.VMEM((seq, qw // 2), F32),
            pltpu.VMEM((seq // 4, seq), F32),
            dma((10,)),
            dma((16,)),
            dma((16, far)),
            dma((8,)),
            dma((8, far)),
            dma((2, 9)),
            dma((2, 9)),
            dma((2, 4)),
            dma((2, 4)),
            dma((2, 6)),
            dma((2, 6)),
        ],
        compiler_params=pltpu.CompilerParams(
            collective_id=0, has_side_effects=True, vmem_limit_bytes=66_000_000
        ),
    )(tokens, gains, lam, cos, sin, wq, wk, wv, ws, wo, wg, wu, wd)


def solution(mesh):
    placed = (
        P(("grp", "fs", "tp"), None),
        P(),
        P("fs", "tp"),
        P("fs", "tp"),
        P("fs", "tp"),
        P("fs", "tp"),
        P("tp", "fs"),
        P("fs", "tp"),
        P("fs", "tp"),
        P("tp", "fs"),
    )
    nf, nt = mesh.shape["fs"], mesh.shape["tp"]
    assert mesh.shape["grp"] % 2 == 0 and nt == 8 and nf % 2 == 0
    return jax.shard_map(
        functools.partial(layer, nf, nt // 2),
        mesh=mesh,
        in_specs=placed,
        out_specs=P(("grp", "fs", "tp"), None),
        check_vma=False,
    )
```

```python
import functools

import jax
import jax.numpy as jnp
import numpy as np
from jax import lax
from jax.experimental import pallas as pl
from jax.experimental.pallas import tpu as pltpu
from jax.sharding import PartitionSpec as P

H = 8
BLOCK = 128
norm_epsilon = 1e-06
group_epsilon = 0.01
MESH = pl.DeviceIdType.MESH
F32 = jnp.float32
BF16 = jnp.bfloat16


def mod(a, n):
    return lax.rem(a + n, n)


def rms(matrix):
    return matrix * lax.rsqrt(jnp.mean(matrix * matrix, axis=-1, keepdims=True) + norm_epsilon)


def silu(v):
    return v / (1.0 + jnp.exp(-v))


def kernel(
    nf,
    nx,
    tok,
    gains,
    lam_ref,
    cos_hbm,
    sin_hbm,
    wq,
    wk,
    wv,
    ws,
    wo,
    wg,
    wu,
    wd,
    out,
    w1,
    w2,
    w3,
    w4,
    xn,
    xw,
    acc,
    qb,
    kb,
    vb,
    gp,
    hid,
    part,
    sib_in,
    stage,
    pass_in,
    from_left,
    from_right,
    am,
    cos,
    sin,
    decay,
    local_sem,
    z_send,
    z_recv,
    y_send,
    y_recv,
    g_send,
    g_recv,
    s_send,
    s_recv,
    r_send,
    r_recv,
):
    rows, width = tok.shape
    seq = xn.shape[0]
    half = width // 2
    quarter = seq // 4
    me = lax.axis_index("fs")
    tp = lax.axis_index("tp")
    group = lax.axis_index("grp")
    x = tp // 2
    core = lax.rem(tp, 2)
    plane = lax.rem(group, 2)
    up = {"fs": mod(me + 1, nf)}
    down = {"fs": mod(me - 1, nf)}
    pair = {"grp": group + 1 - 2 * plane}
    sib = {"tp": 2 * x + 1 - core}
    right = {"tp": 2 * mod(x + 1, nx) + core}
    left = {"tp": 2 * mod(x - 1, nx) + core}

    def copy(src, dst, send, recv, device):
        return pltpu.make_async_remote_copy(
            src_ref=src,
            dst_ref=dst,
            send_sem=send,
            recv_sem=recv,
            device_id=device,
            device_id_type=MESH,
        )

    kd = wq.shape[0]
    mine = pl.ds(pl.multiple_of(me * kd, kd), kd)
    mine_cols = pl.ds(pl.multiple_of(me * kd, kd), kd)
    qw, vw, ff = wq.shape[1], wv.shape[1], wg.shape[1]
    locals_ = [
        (wq, w1.at[mine, 0:qw]),
        (wk, w1.at[mine, qw : 2 * qw]),
        (wv, w1.at[mine, 2 * qw : 2 * qw + vw]),
        (ws, w1.at[mine, 2 * qw + vw : 2 * qw + 2 * vw]),
        (wo, w2.at[:, mine_cols]),
        (wg, w3.at[mine, 0:ff]),
        (wu, w3.at[mine, ff : 2 * ff]),
        (wd, w4.at[:, mine_cols]),
        (cos_hbm, cos),
        (sin_hbm, sin),
    ]
    loads = [
        pltpu.make_async_copy(src, dst, local_sem.at[i]) for i, (src, dst) in enumerate(locals_)
    ]
    for load in loads:
        load.start()

    barrier = pltpu.get_barrier_semaphore()
    for device in (up, down, pair, sib, right, left):
        pl.semaphore_signal(barrier, inc=1, device_id=device, device_id_type=MESH)

    own = pl.multiple_of(tp * rows, rows)

    def norm_in(i, carry):
        at = pl.multiple_of(i * 16, 16)
        value = rms(tok[pl.ds(at, 16), :].astype(F32)) * gains[0:1, :]
        xn[pl.ds(own + at, 16), :] = value.astype(BF16)
        return carry

    lax.fori_loop(0, rows // 16, norm_in, 0)
    pl.semaphore_wait(barrier, 6)

    def third(total):
        return total // 3 // 16 * 16 + (16 if total // 3 % 16 else 0)

    pieces = (4, 2, 2, 2)
    owns = (2, 1, 1, 1)

    def place(a, owner, piece, plane_, rows_half=None):
        ref = (w1, w2, w3, w4)[a]
        if a in (0, 2):
            w = ref.shape[1] // 3 // owns[a]
            start, count = owner * kd, kd
            if rows_half is not None:
                count = kd // 2
                start = start + rows_half * count
            r = pl.ds(pl.multiple_of(start, kd // 2), count)
            if piece < owns[a]:
                at = pl.multiple_of(plane_ * 2 * w * owns[a] + piece * w, 128)
            else:
                at = piece * w
            return ref.at[r, pl.ds(at, w)]
        t = third(ref.shape[0])
        mid = ref.shape[0] - 2 * t
        r = pl.ds(pl.multiple_of(plane_ * (t + mid), 16), t) if piece == 0 else pl.ds(t, mid)
        return ref.at[r, pl.ds(pl.multiple_of(owner * kd, kd), kd)]

    def z_index(a, d, piece):
        return 2 * sum(pieces[:a]) + d * pieces[a] + piece

    def y_index(a, d, piece):
        return 2 * sum(owns[:a]) + d * owns[a] + piece

    def owner_of(d, s):
        return mod(me - s, nf) if d == 0 else lax.rem(me + s, nf)

    far = nf // 2

    def z_copy(a, d, piece, s, rows_half=None):
        src = place(a, owner_of(d, s - 1), piece, plane, rows_half)
        k = z_index(a, d, piece)
        return copy(src, src, z_send.at[k], z_recv.at[k, s - 1], up if d == 0 else down)

    def z_arrived(a, d, piece, s, rows_half=None):
        dst = place(a, owner_of(d, s), piece, plane, rows_half)
        k = z_index(a, d, piece)
        copy(dst, dst, z_send.at[k], z_recv.at[k, s - 1], up if d == 0 else down).wait_recv()

    def y_copy(a, d, piece, s, rows_half=None):
        src = place(a, owner_of(d, s), piece, plane, rows_half)
        k = y_index(a, d, piece)
        return copy(src, src, y_send.at[k], y_recv.at[k, s - 1], pair)

    def y_arrived(a, d, piece, s, rows_half=None):
        dst = place(a, owner_of(d, s), piece, 1 - plane, rows_half)
        k = y_index(a, d, piece)
        copy(dst, dst, y_send.at[k], y_recv.at[k, s - 1], pair).wait_recv()

    def last_half(a, d):
        return d if a in (0, 2) else None

    def has_last(a, d):
        return a in (0, 2) or (a == 1 and d == 0) or (a == 3 and d == 1)

    def begin(a):
        for piece in range(pieces[a]):
            for d in (0, 1):
                z_copy(a, d, piece, 1).start()

    def forward(a, s, piece):
        for d in (0, 1):
            here = s < far or has_last(a, d)
            part_of = last_half(a, d) if s == far else None
            if here:
                z_arrived(a, d, piece, s, part_of)
                z_copy(a, d, piece, s, part_of).wait_send()
            if s < far - 1:
                z_copy(a, d, piece, s + 1).start()
            elif s == far - 1 and has_last(a, d):
                z_copy(a, d, piece, far, last_half(a, d)).start()
            if piece < owns[a]:
                if s > 1:
                    y_copy(a, d, piece, s - 1).wait_send()
                if here:
                    y_copy(a, d, piece, s, part_of).start()

    def slot(*items):
        for piece in range(4):
            for a, s in items:
                if piece < pieces[a]:
                    forward(a, s, piece)

    def y_all(a, s):
        for piece in range(owns[a]):
            for d in (0, 1):
                if s < far or has_last(a, d):
                    y_arrived(a, d, piece, s, last_half(a, d) if s == far else None)

    def y_drain(a):
        for piece in range(owns[a]):
            for d in (0, 1):
                if has_last(a, d):
                    y_copy(a, d, piece, far, last_half(a, d)).wait_send()

    def gather(n, ref, at, count):
        at_left, at_right, at_far = mod(x - 1, nx), mod(x + 1, nx), mod(x + 2, nx)
        lo, hi = pl.ds(0, half), pl.ds(half, half)
        every = pl.ds(0, width)

        def whole(xx, cc, cols=every):
            return ref.at[pl.ds(pl.multiple_of((2 * xx + cc) * rows + at, count), count), cols]

        def send(k, xx, cols, device):
            src = whole(xx, core, cols)
            return copy(src, src, g_send.at[n, k], g_recv.at[n, k], device)

        def arrived(k, xx, cc, cols):
            dst = whole(xx, cc, cols)
            copy(dst, dst, g_send.at[n, k], g_recv.at[n, k], sib).wait_recv()

        sends = []

        def go(*args):
            s = send(*args)
            s.start()
            sends.append(s)

        def first():
            go(1, x, every, right)
            go(2, x, every, left)
            go(0, x, every, sib)

        def second():
            arrived(1, at_left, core, every)
            go(3, at_left, lo, right)
            go(4, at_left, every, sib)
            arrived(2, at_right, core, every)
            go(5, at_right, hi, left)
            go(6, at_right, every, sib)

        def third_():
            arrived(3, at_far, core, lo)
            go(7, at_far, lo, sib)
            arrived(5, at_far, core, hi)
            go(8, at_far, hi, sib)

        def own_chip():
            arrived(0, x, 1 - core, every)

        def near():
            arrived(4, at_left, 1 - core, every)
            arrived(6, at_right, 1 - core, every)

        def rest():
            arrived(7, at_far, 1 - core, lo)
            arrived(8, at_far, 1 - core, hi)

        def drain():
            for s in sends:
                s.wait_send()

        return first, second, third_, own_chip, near, rest, drain

    for load in loads[:4]:
        load.wait()
    begin(0)
    first, second, third_, own_chip, near, rest, drain1 = gather(0, xn, 0, rows)
    first()

    lam = lam_ref[0:1, 0:1]
    dn = lax.broadcasted_iota(jnp.int32, decay.shape, 0) + (seq - quarter)
    dm = lax.broadcasted_iota(jnp.int32, decay.shape, 1)
    dist = (dn - dm).astype(F32)
    decay[...] = jnp.where(dist >= 0.0, jnp.exp(lam * jnp.maximum(dist, 0.0)), 0.0)
    for load in loads[4:]:
        load.wait()

    def k_slice(owner):
        return pl.ds(pl.multiple_of(owner * kd, kd), kd)

    def tiled(tiles, body):
        n = acc.shape[1] // 2

        def step(i, carry):
            r = pl.ds(pl.multiple_of(i // 2 * quarter, quarter), quarter)
            body(r, pl.ds(pl.multiple_of(lax.rem(i, 2) * n, n), n))
            return carry

        lax.fori_loop(2 * tiles[0], 2 * tiles[1], step, 0)

    def add_own(tiles):
        def body(r, c):
            acc[r, c] = jnp.dot(
                xn[r, k_slice(me)], w1[k_slice(me), c], preferred_element_type=F32
            )

        tiled(tiles, body)

    def add_two(s, tiles):
        a, b = k_slice(owner_of(0, s)), k_slice(owner_of(1, s))

        def body(r, c):
            acc[r, c] = (
                acc[r, c]
                + jnp.dot(xn[r, a], w1[a, c], preferred_element_type=F32)
                + jnp.dot(xn[r, b], w1[b, c], preferred_element_type=F32)
            )

        tiled(tiles, body)

    def slot_and_add(s, add):
        forward(0, s, 0)
        forward(1, s, 0)
        add((0, 1))
        forward(0, s, 1)
        add((1, 2))
        forward(0, s, 2)
        forward(1, s, 1)
        add((2, 3))
        forward(0, s, 3)
        add((3, 4))

    begin(1)
    slot((0, 1), (1, 1))
    second()
    slot((0, 2), (1, 2))
    own_chip()
    third_()
    near()
    rest()
    slot_and_add(3, add_own)
    y_all(0, 1)
    slot_and_add(4, functools.partial(add_two, 1))

    for s in (5, 6, 7):
        y_all(0, s - 3)
        slot_and_add(s, functools.partial(add_two, s - 3))
    begin(2)
    begin(3)
    y_all(0, far - 3)
    add_two(far - 3, (0, 4))
    slot((0, far), (1, far))
    y_all(0, far - 2)
    add_two(far - 2, (0, 4))
    y_all(0, far - 1)
    add_two(far - 1, (0, 4))
    y_all(0, far)
    far_slice = k_slice(owner_of(0, far))

    key_scale = float(qw) ** -0.5
    hq = qw // 2

    def finish(i, carry):
        r = pl.ds(pl.multiple_of(i * quarter, quarter), quarter)
        total = acc[r, :] + jnp.dot(xn[r, far_slice], w1[far_slice, :], preferred_element_type=F32)
        c, s = cos[r, :], sin[r, :]
        for ref, at, scale in ((qb, 0, None), (kb, qw, key_scale)):
            a, b = total[:, at : at + hq], total[:, at + hq : at + qw]
            first_half = a * c - b * s
            second_half = a * s + b * c
            if scale is not None:
                first_half, second_half = first_half * scale, second_half * scale
            ref[r, 0:hq] = first_half.astype(BF16)
            ref[r, hq:qw] = second_half.astype(BF16)
        vb[r, :] = total[:, 2 * qw : 2 * qw + vw].astype(BF16)
        acc[r, 2 * qw + vw :] = total[:, 2 * qw + vw :]
        return carry

    lax.fori_loop(0, 4, finish, 0)
    slot((2, 1), (3, 1))

    def retain(i):
        r = slice(i * quarter, (i + 1) * quarter)
        seen = (i + 1) * quarter
        scores = lax.dot_general(
            qb[r, :], kb[0:seen, :], (((1,), (1,)), ((), ())), preferred_element_type=F32
        )
        weighted = (scores * decay[:, seq - seen :]).astype(BF16)
        retained = jnp.dot(weighted, vb[0:seen, :], preferred_element_type=F32)
        centred = retained - jnp.mean(retained, axis=-1, keepdims=True)
        normalized = centred * lax.rsqrt(
            jnp.mean(centred * centred, axis=-1, keepdims=True) + group_epsilon
        )
        gp[r, :] = (silu(acc[r, 2 * qw + vw :]) * normalized).astype(BF16)

    retain(0)
    retain(1)
    retain(2)
    retain(3)
    for s in range(1, far + 1):
        y_all(1, s)
    slot((2, 2), (3, 2))

    lo, hi = slice(0, half), slice(half, width)
    chunk = rows // 2
    near_x = (mod(x + 2, nx), mod(x + 1, nx), mod(x - 1, nx), x)

    class Reduce:
        def __init__(self, n, lhs, weight):
            self.n, self.lhs, self.weight = n, lhs, weight
            self.sends, self.sib, self.got = [], {}, {}

        def project(self, k):
            n, xx = self.n, near_x[k]
            r = pl.ds(pl.multiple_of(2 * xx * rows, 2 * rows), 2 * rows)
            cols = width // 4

            def body(j, carry):
                at = pl.ds(pl.multiple_of(j * cols, cols), cols)
                product = jnp.dot(self.lhs[r, :], self.weight[:, at], preferred_element_type=F32)
                part[r, at] = product.astype(BF16)
                return carry

            lax.fori_loop(0, 4, body, 0)
            s = copy(
                part.at[pl.ds(pl.multiple_of((2 * xx + 1 - core) * rows, rows), rows), :],
                sib_in.at[n, k],
                s_send.at[n, k],
                s_recv.at[n, k],
                sib,
            )
            s.start()
            self.sends.append(s)
            self.sib[k] = s

        def paired(self, k):
            self.sib[k].wait_recv()

        def pre(self, k, ch, cols):
            at = pl.multiple_of((2 * near_x[k] + core) * rows + ch * chunk, chunk)
            r = slice(ch * chunk, (ch + 1) * chunk)
            return part[pl.ds(at, chunk), cols].astype(F32) + sib_in[self.n, k, r, cols].astype(F32)

        def ship(self, name, ch, slot_, value, cols, dst, device):
            n = self.n
            i = ch * 6 + ("pr", "pl", "dr", "dl", "sr", "sl").index(name)
            r = pl.ds(ch * chunk, chunk)
            stage[n, slot_, r, cols] = value.astype(BF16)
            s = copy(stage.at[n, slot_, r, cols], dst, r_send.at[n, i], r_recv.at[n, i], device)
            s.start()
            self.sends.append(s)
            self.got[name, ch] = s

        def passes(self, ch):
            n, r = self.n, pl.ds(ch * chunk, chunk)
            self.ship("pr", ch, 0, self.pre(0, ch, hi), hi, pass_in.at[n, 0, r], right)
            self.ship("pl", ch, 0, self.pre(0, ch, lo), lo, pass_in.at[n, 1, r], left)

        def direct_right(self, ch):
            dst = from_left.at[self.n, pl.ds(ch * chunk, chunk), lo]
            self.ship("dr", ch, 1, self.pre(1, ch, lo), lo, dst, right)

        def direct_left(self, ch):
            dst = from_right.at[self.n, pl.ds(ch * chunk, chunk), hi]
            self.ship("dl", ch, 2, self.pre(2, ch, hi), hi, dst, left)

        def sums(self, ch):
            n, r = self.n, pl.ds(ch * chunk, chunk)
            self.got["pr", ch].wait_recv()
            value = self.pre(1, ch, hi) + pass_in[n, 0, r].astype(F32)
            self.ship("sr", ch, 1, value, hi, from_left.at[n, r, hi], right)
            self.got["pl", ch].wait_recv()
            value = self.pre(2, ch, lo) + pass_in[n, 1, r].astype(F32)
            self.ship("sl", ch, 2, value, lo, from_right.at[n, r, lo], left)

        def arrive(self, ch):
            for name in ("dr", "dl", "sr", "sl"):
                self.got[name, ch].wait_recv()

        def total(self, at, count):
            n, r = self.n, pl.ds(at, count)
            base = pl.multiple_of((2 * x + core) * rows + at, count)
            return (
                (part[pl.ds(base, count), :].astype(F32) + sib_in[n, 3, r, :].astype(F32))
                + from_left[n, r, :].astype(F32)
                + from_right[n, r, :].astype(F32)
            )

        def drain(self):
            for s in self.sends:
                s.wait_send()

    one = Reduce(0, gp, w2)
    one.project(0)
    one.project(1)
    one.paired(0)
    one.passes(0)
    one.passes(1)
    one.project(2)
    one.paired(1)
    one.direct_right(0)
    one.direct_right(1)
    one.project(3)
    one.paired(2)
    one.direct_left(0)
    one.direct_left(1)
    slot((2, 3), (3, 3))
    one.sums(0)
    slot((2, 4), (3, 4))
    one.sums(1)
    one.paired(3)
    slot((2, 5), (3, 5))

    def mixed(i, carry):
        at = pl.multiple_of(i * 16, 16)
        after = tok[pl.ds(at, 16), :].astype(F32) + rms(one.total(at, 16)) * gains[1:2, :]
        am[pl.ds(at, 16), :] = after
        xw[pl.ds(pl.multiple_of(own + at, 16), 16), :] = (rms(after) * gains[2:3, :]).astype(BF16)
        return carry

    per = chunk // 16
    two = [gather(1, xw, 0, chunk), gather(2, xw, chunk, chunk)]
    one.arrive(0)
    lax.fori_loop(0, per, mixed, 0)
    two[0][0]()
    slot((2, 6), (3, 6))
    one.arrive(1)
    lax.fori_loop(per, 2 * per, mixed, 0)
    two[1][0]()
    slot((2, 7), (3, 7))
    two[0][1]()
    slot((2, 8), (3, 8))
    two[1][1]()
    one.drain()
    for s in range(1, far + 1):
        y_all(2, s)

    def feed(k):
        r = pl.ds(pl.multiple_of(2 * near_x[k] * rows, 2 * rows), 2 * rows)
        both = jnp.dot(xw[r, :], w3[...], preferred_element_type=F32)
        hid[r, :] = (silu(both[:, 0:ff]) * both[:, ff:]).astype(BF16)

    two[0][3]()
    two[1][3]()
    feed(3)
    for s in range(1, far + 1):
        y_all(3, s)
    last_one = Reduce(1, hid, w4)
    two[0][4]()
    two[1][4]()
    feed(1)
    last_one.project(1)
    two[0][2]()
    feed(2)
    last_one.project(2)
    last_one.paired(1)
    last_one.direct_right(0)
    last_one.direct_right(1)
    last_one.paired(2)
    last_one.direct_left(0)
    last_one.direct_left(1)
    two[1][2]()
    last_one.project(3)
    two[0][5]()
    two[1][5]()
    feed(0)
    last_one.project(0)
    last_one.paired(0)
    last_one.passes(0)
    last_one.passes(1)
    last_one.paired(3)
    last_one.sums(0)
    last_one.sums(1)

    def last(i, carry):
        at = pl.multiple_of(i * 16, 16)
        r = pl.ds(at, 16)
        out[r, :] = (am[r, :] + rms(last_one.total(at, 16)) * gains[3:4, :]).astype(BF16)
        return carry

    last_one.arrive(0)
    lax.fori_loop(0, per, last, 0)
    last_one.arrive(1)
    lax.fori_loop(per, 2 * per, last, 0)
    drain1()
    two[0][6]()
    two[1][6]()
    last_one.drain()
    for a in range(4):
        y_drain(a)


def layer(nf, nx, tokens, gains, wq, wk, wv, ws, wo, wg, wu, wd):
    rows, width = tokens.shape
    seq = rows * 2 * nx
    qw, vw, ff = wq.shape[1], wv.shape[1], wg.shape[1]
    frequency = 10000.0 ** (-np.linspace(0.0, 1.0, qw // 2))
    angles = np.arange(seq, dtype=np.float64)[:, None] * frequency[None, :]
    cos = jnp.asarray(np.cos(angles).astype(np.float32))
    sin = jnp.asarray(np.sin(angles).astype(np.float32))
    head = lax.axis_index("tp").astype(F32)
    lam = -(4.0 / BLOCK) * (BLOCK / (32.0 * seq)) ** (head / (H - 1))
    lam = jnp.full((8, 128), lam, F32)
    vmem = pl.BlockSpec(memory_space=pltpu.VMEM)
    hbm = pl.BlockSpec(memory_space=pl.ANY)
    dma = pltpu.SemaphoreType.DMA
    far = nf // 2
    half = width // 2
    n1 = 2 * qw + 2 * vw
    return pl.pallas_call(
        functools.partial(kernel, nf, nx),
        out_shape=jax.ShapeDtypeStruct((rows, width), BF16),
        in_specs=[vmem] * 3 + [hbm] * 10,
        out_specs=vmem,
        scratch_shapes=[
            pltpu.VMEM((width, n1), BF16),
            pltpu.VMEM((wo.shape[0], width), BF16),
            pltpu.VMEM((width, 2 * ff), BF16),
            pltpu.VMEM((wd.shape[0], width), BF16),
            pltpu.VMEM((seq, width), BF16),
            pltpu.VMEM((seq, width), BF16),
            pltpu.VMEM((seq, n1), F32),
            pltpu.VMEM((seq, qw), BF16),
            pltpu.VMEM((seq, qw), BF16),
            pltpu.VMEM((seq, vw), BF16),
            pltpu.VMEM((seq, vw), BF16),
            pltpu.VMEM((seq, ff), BF16),
            pltpu.VMEM((seq, width), BF16),
            pltpu.VMEM((2, nx, rows, width), BF16),
            pltpu.VMEM((2, 3, rows, width), BF16),
            pltpu.VMEM((2, 2, rows, half), BF16),
            pltpu.VMEM((2, rows, width), BF16),
            pltpu.VMEM((2, rows, width), BF16),
            pltpu.VMEM((rows, width), F32),
            pltpu.VMEM((seq, qw // 2), F32),
            pltpu.VMEM((seq, qw // 2), F32),
            pltpu.VMEM((seq // 4, seq), F32),
            dma((10,)),
            dma((20,)),
            dma((20, far)),
            dma((10,)),
            dma((10, far)),
            dma((3, 9)),
            dma((3, 9)),
            dma((2, 4)),
            dma((2, 4)),
            dma((2, 12)),
            dma((2, 12)),
        ],
        compiler_params=pltpu.CompilerParams(
            collective_id=0, has_side_effects=True, vmem_limit_bytes=66_000_000
        ),
    )(tokens, gains, lam, cos, sin, wq, wk, wv, ws, wo, wg, wu, wd)


def solution(mesh):
    placed = (
        P(("grp", "fs", "tp"), None),
        P(),
        P("fs", "tp"),
        P("fs", "tp"),
        P("fs", "tp"),
        P("fs", "tp"),
        P("tp", "fs"),
        P("fs", "tp"),
        P("fs", "tp"),
        P("tp", "fs"),
    )
    nf, nt = mesh.shape["fs"], mesh.shape["tp"]
    assert mesh.shape["grp"] % 2 == 0 and nt == 8 and nf % 2 == 0
    return jax.shard_map(
        functools.partial(layer, nf, nt // 2),
        mesh=mesh,
        in_specs=placed,
        out_specs=P(("grp", "fs", "tp"), None),
        check_vma=False,
    )
```

```python
import functools

import jax
import jax.numpy as jnp
import numpy as np
from jax import lax
from jax.experimental import pallas as pl
from jax.experimental.pallas import tpu as pltpu
from jax.sharding import PartitionSpec as P

H = 8
BLOCK = 128
norm_epsilon = 1e-06
group_epsilon = 0.01
MESH = pl.DeviceIdType.MESH
F32 = jnp.float32
BF16 = jnp.bfloat16


def mod(a, n):
    return lax.rem(a + n, n)


def rms(matrix):
    return matrix * lax.rsqrt(jnp.mean(matrix * matrix, axis=-1, keepdims=True) + norm_epsilon)


def silu(v):
    return v / (1.0 + jnp.exp(-v))


def kernel(
    nf,
    nx,
    tok,
    gains,
    lam_ref,
    turn_hbm,
    base_ref,
    wq,
    wk,
    wv,
    ws,
    wo,
    wg,
    wu,
    wd,
    out,
    w1,
    w2,
    w3,
    w4,
    xn,
    xw,
    acc,
    qb,
    kb,
    vb,
    gp,
    hid,
    part,
    sib_in,
    stage,
    pass_in,
    from_left,
    from_right,
    am,
    turn,
    decay,
    local_sem,
    z_send,
    z_recv,
    y_send,
    y_recv,
    g_send,
    g_recv,
    s_send,
    s_recv,
    r_send,
    r_recv,
):
    rows, width = tok.shape
    seq = xn.shape[0]
    half = width // 2
    quarter = seq // 4
    me = lax.axis_index("fs")
    tp = lax.axis_index("tp")
    group = lax.axis_index("grp")
    x = tp // 2
    core = lax.rem(tp, 2)
    plane = lax.rem(group, 2)
    up = {"fs": mod(me + 1, nf)}
    down = {"fs": mod(me - 1, nf)}
    pair = {"grp": group + 1 - 2 * plane}
    sib = {"tp": 2 * x + 1 - core}
    right = {"tp": 2 * mod(x + 1, nx) + core}
    left = {"tp": 2 * mod(x - 1, nx) + core}

    def copy(src, dst, send, recv, device):
        return pltpu.make_async_remote_copy(
            src_ref=src,
            dst_ref=dst,
            send_sem=send,
            recv_sem=recv,
            device_id=device,
            device_id_type=MESH,
        )

    kd = wq.shape[0]
    mine = pl.ds(pl.multiple_of(me * kd, kd), kd)
    mine_cols = pl.ds(pl.multiple_of(me * kd, kd), kd)
    qw, vw, ff = wq.shape[1], wv.shape[1], wg.shape[1]
    locals_ = [
        (wq, w1.at[mine, 0:qw]),
        (wk, w1.at[mine, qw : 2 * qw]),
        (wv, w1.at[mine, 2 * qw : 2 * qw + vw]),
        (ws, w1.at[mine, 2 * qw + vw : 2 * qw + 2 * vw]),
        (wo, w2.at[:, mine_cols]),
        (wg, w3.at[mine, 0:ff]),
        (wu, w3.at[mine, ff : 2 * ff]),
        (wd, w4.at[:, mine_cols]),
        (turn_hbm, turn),
    ]
    loads = [
        pltpu.make_async_copy(src, dst, local_sem.at[i]) for i, (src, dst) in enumerate(locals_)
    ]
    for load in loads:
        load.start()

    barrier = pltpu.get_barrier_semaphore()
    for device in (up, down, pair, sib, right, left):
        pl.semaphore_signal(barrier, inc=1, device_id=device, device_id_type=MESH)

    own = pl.multiple_of(tp * rows, rows)

    def norm_in(i, carry):
        at = pl.multiple_of(i * 16, 16)
        value = rms(tok[pl.ds(at, 16), :].astype(F32)) * gains[0:1, :]
        xn[pl.ds(own + at, 16), :] = value.astype(BF16)
        return carry

    lax.fori_loop(0, rows // 16, norm_in, 0)
    pl.semaphore_wait(barrier, 6)

    def third(total):
        return total // 3 // 16 * 16 + (16 if total // 3 % 16 else 0)

    pieces = (4, 2, 2, 2)
    owns = (2, 1, 1, 1)

    def place(a, owner, piece, plane_, rows_half=None):
        ref = (w1, w2, w3, w4)[a]
        if a in (0, 2):
            w = ref.shape[1] // 3 // owns[a]
            start, count = owner * kd, kd
            if rows_half is not None:
                count = kd // 2
                start = start + rows_half * count
            r = pl.ds(pl.multiple_of(start, kd // 2), count)
            if piece < owns[a]:
                at = pl.multiple_of(plane_ * 2 * w * owns[a] + piece * w, 128)
            else:
                at = piece * w
            return ref.at[r, pl.ds(at, w)]
        t = third(ref.shape[0])
        mid = ref.shape[0] - 2 * t
        r = pl.ds(pl.multiple_of(plane_ * (t + mid), 16), t) if piece == 0 else pl.ds(t, mid)
        return ref.at[r, pl.ds(pl.multiple_of(owner * kd, kd), kd)]

    def z_index(a, d, piece):
        return 2 * sum(pieces[:a]) + d * pieces[a] + piece

    def y_index(a, d, piece):
        return 2 * sum(owns[:a]) + d * owns[a] + piece

    def owner_of(d, s):
        return mod(me - s, nf) if d == 0 else lax.rem(me + s, nf)

    far = nf // 2

    def z_copy(a, d, piece, s, rows_half=None):
        src = place(a, owner_of(d, s - 1), piece, plane, rows_half)
        k = z_index(a, d, piece)
        return copy(src, src, z_send.at[k], z_recv.at[k, s - 1], up if d == 0 else down)

    def z_arrived(a, d, piece, s, rows_half=None):
        dst = place(a, owner_of(d, s), piece, plane, rows_half)
        k = z_index(a, d, piece)
        copy(dst, dst, z_send.at[k], z_recv.at[k, s - 1], up if d == 0 else down).wait_recv()

    def y_sem(a, d, s):
        return y_recv.at[d * far + s - 1] if a == 0 else y_recv.at[2 * far + a - 1]

    def y_copy(a, d, piece, s, rows_half=None):
        src = place(a, owner_of(d, s), piece, plane, rows_half)
        return copy(src, src, y_send.at[y_index(a, d, piece)], y_sem(a, d, s), pair)

    def last_half(a, d):
        return d if a in (0, 2) else None

    def has_last(a, d):
        return a in (0, 2) or (a == 1 and d == 0) or (a == 3 and d == 1)

    def begin(a):
        for piece in range(pieces[a]):
            for d in (0, 1):
                z_copy(a, d, piece, 1).start()

    def forward(a, s, piece):
        for d in (0, 1):
            here = s < far or has_last(a, d)
            part_of = last_half(a, d) if s == far else None
            if here:
                z_arrived(a, d, piece, s, part_of)
                z_copy(a, d, piece, s, part_of).wait_send()
            if s < far - 1:
                z_copy(a, d, piece, s + 1).start()
            elif s == far - 1 and has_last(a, d):
                z_copy(a, d, piece, far, last_half(a, d)).start()
            if piece < owns[a]:
                if s > 1:
                    y_copy(a, d, piece, s - 1).wait_send()
                if here:
                    y_copy(a, d, piece, s, part_of).start()

    def slot(*items):
        for piece in range(4):
            for a, s in items:
                if piece < pieces[a]:
                    forward(a, s, piece)

    def y_step(s):
        w = w1.shape[1] // 3
        for d in (0, 1):
            count = kd if s < far else kd // 2
            start = owner_of(d, s) * kd + (0 if s < far else d * count)
            at = pl.multiple_of((1 - plane) * 2 * w, 128)
            dst = w1.at[pl.ds(pl.multiple_of(start, kd // 2), count), pl.ds(at, w)]
            copy(dst, dst, y_send.at[0], y_sem(0, d, s), pair).wait_recv()

    def y_whole(a):
        ref = (w1, w2, w3, w4)[a]
        n = (nf - 1) * kd
        if a == 2:
            w = ref.shape[1] // 3
            dst = ref.at[0:n, pl.ds(pl.multiple_of((1 - plane) * 2 * w, 128), w)]
        else:
            t = third(ref.shape[0])
            dst = ref.at[pl.ds(pl.multiple_of((1 - plane) * (ref.shape[0] - t), 16), t), 0:n]
        copy(dst, dst, y_send.at[0], y_sem(a, 0, 1), pair).wait_recv()

    def y_drain(a):
        for piece in range(owns[a]):
            for d in (0, 1):
                if has_last(a, d):
                    y_copy(a, d, piece, far, last_half(a, d)).wait_send()

    def gather(n, ref, at, count):
        at_left, at_right, at_far = mod(x - 1, nx), mod(x + 1, nx), mod(x + 2, nx)
        lo, hi = pl.ds(0, half), pl.ds(half, half)
        every = pl.ds(0, width)

        def whole(xx, cc, cols=every):
            return ref.at[pl.ds(pl.multiple_of((2 * xx + cc) * rows + at, count), count), cols]

        def send(k, xx, cols, device):
            src = whole(xx, core, cols)
            return copy(src, src, g_send.at[n, k], g_recv.at[n, k], device)

        def arrived(k, xx, cc, cols):
            dst = whole(xx, cc, cols)
            copy(dst, dst, g_send.at[n, k], g_recv.at[n, k], sib).wait_recv()

        sends = []

        def go(*args):
            s = send(*args)
            s.start()
            sends.append(s)

        def first():
            go(1, x, every, right)
            go(2, x, every, left)
            go(0, x, every, sib)

        def second():
            arrived(1, at_left, core, every)
            go(3, at_left, lo, right)
            go(4, at_left, every, sib)
            arrived(2, at_right, core, every)
            go(5, at_right, hi, left)
            go(6, at_right, every, sib)

        def third_():
            arrived(3, at_far, core, lo)
            go(7, at_far, lo, sib)
            arrived(5, at_far, core, hi)
            go(8, at_far, hi, sib)

        def own_chip():
            arrived(0, x, 1 - core, every)

        def near():
            arrived(4, at_left, 1 - core, every)
            arrived(6, at_right, 1 - core, every)

        def rest():
            arrived(7, at_far, 1 - core, lo)
            arrived(8, at_far, 1 - core, hi)

        def drain():
            for s in sends:
                s.wait_send()

        return first, second, third_, own_chip, near, rest, drain

    for load in loads[:4]:
        load.wait()
    begin(0)
    first, second, third_, own_chip, near, rest, drain1 = gather(0, xn, 0, rows)
    first()

    lam = lam_ref[pl.ds(tp, 1), 0:1]
    dn = lax.broadcasted_iota(jnp.int32, decay.shape, 0) + (seq - quarter)
    dm = lax.broadcasted_iota(jnp.int32, decay.shape, 1)
    dist = (dn - dm).astype(F32)
    decay[...] = jnp.where(dist >= 0.0, jnp.exp(lam * jnp.maximum(dist, 0.0)), 0.0)
    for load in loads[4:]:
        load.wait()

    def k_slice(owner):
        return pl.ds(pl.multiple_of(owner * kd, kd), kd)

    def tiled(tiles, body):
        n = acc.shape[1] // 2

        def step(i, carry):
            r = pl.ds(pl.multiple_of(i // 2 * quarter, quarter), quarter)
            body(r, pl.ds(pl.multiple_of(lax.rem(i, 2) * n, n), n))
            return carry

        lax.fori_loop(2 * tiles[0], 2 * tiles[1], step, 0)

    def add_own(tiles):
        def body(r, c):
            acc[r, c] = jnp.dot(
                xn[r, k_slice(me)], w1[k_slice(me), c], preferred_element_type=F32
            )

        tiled(tiles, body)

    def add_two(s, tiles):
        a, b = k_slice(owner_of(0, s)), k_slice(owner_of(1, s))

        def body(r, c):
            acc[r, c] = (
                acc[r, c]
                + jnp.dot(xn[r, a], w1[a, c], preferred_element_type=F32)
                + jnp.dot(xn[r, b], w1[b, c], preferred_element_type=F32)
            )

        tiled(tiles, body)

    def slot_and_add(s, adds):
        for piece in range(4):
            forward(0, s, piece)
            if piece < 3:
                for waits, add, tiles in adds[piece]:
                    if waits:
                        y_step(waits)
                    add(tiles)
        forward(1, s, 0)
        forward(1, s, 1)

    polls = [(s, piece) for s in range(1, far + 1) for piece in (0, 1)]

    def poll():
        s, piece = polls.pop(0)
        forward(2, s, piece)
        forward(3, s, piece)

    def two_of(s, tiles, wait=True):
        return s if wait else 0, functools.partial(add_two, s), tiles

    begin(1)
    slot((0, 1))
    forward(1, 1, 0)
    forward(1, 1, 1)
    second()
    slot((0, 2))
    forward(1, 2, 0)
    forward(1, 2, 1)
    own_chip()
    third_()
    forward(0, 3, 0)
    forward(0, 3, 1)
    near()
    rest()
    forward(0, 3, 2)
    forward(0, 3, 3)
    forward(1, 3, 0)
    forward(1, 3, 1)
    slot_and_add(4, ([(0, add_own, (0, 4))], [two_of(1, (0, 4))], [two_of(2, (0, 2))]))
    slot_and_add(
        5, ([two_of(2, (2, 4), False)], [two_of(3, (0, 4))], [two_of(4, (0, 2))])
    )
    for s in range(6, far):
        slot_and_add(s, ([two_of(s - 2, (2, 4), False)], [], [two_of(s - 1, (0, 2))]))
    begin(2)
    begin(3)
    slot_and_add(far, ([two_of(far - 2, (2, 4), False)], [], [two_of(far - 1, (0, 2))]))
    add_two(far - 1, (2, 4))
    poll()
    y_step(far)
    far_slice = k_slice(owner_of(0, far))

    key_scale = float(qw) ** -0.5
    hq = qw // 2

    def finish(i, carry):
        r = pl.ds(pl.multiple_of(i * quarter, quarter), quarter)
        total = acc[r, :] + jnp.dot(xn[r, far_slice], w1[far_slice, :], preferred_element_type=F32)
        cb, sb = base_ref[pl.ds(i, 1), :], base_ref[pl.ds(i + 4, 1), :]
        c = cb * turn[0] - sb * turn[1]
        s = sb * turn[0] + cb * turn[1]
        for ref, at, scale in ((qb, 0, None), (kb, qw, key_scale)):
            a, b = total[:, at : at + hq], total[:, at + hq : at + qw]
            first_half = a * c - b * s
            second_half = a * s + b * c
            if scale is not None:
                first_half, second_half = first_half * scale, second_half * scale
            ref[r, 0:hq] = first_half.astype(BF16)
            ref[r, hq:qw] = second_half.astype(BF16)
        vb[r, :] = total[:, 2 * qw : 2 * qw + vw].astype(BF16)
        acc[r, 2 * qw + vw :] = total[:, 2 * qw + vw :]
        return carry

    lax.fori_loop(0, 4, finish, 0)
    poll()

    near_x = (mod(x + 2, nx), mod(x + 1, nx), mod(x - 1, nx), x)

    def retain(k):
        i = near_x[k]
        r = pl.ds(pl.multiple_of(i * quarter, quarter), quarter)
        seen = pl.ds(pl.multiple_of((nx - 1 - i) * quarter, quarter), seq)
        scores = lax.dot_general(
            qb[r, :], kb[...], (((1,), (1,)), ((), ())), preferred_element_type=F32
        )
        weighted = (scores * decay[:, seen]).astype(BF16)
        retained = jnp.dot(weighted, vb[...], preferred_element_type=F32)
        centred = retained - jnp.mean(retained, axis=-1, keepdims=True)
        normalized = centred * lax.rsqrt(
            jnp.mean(centred * centred, axis=-1, keepdims=True) + group_epsilon
        )
        gp[r, :] = (silu(acc[r, 2 * qw + vw :]) * normalized).astype(BF16)

    lo, hi = slice(0, half), slice(half, width)
    chunk = rows // 2

    def blocks_of(items):
        return [
            pl.ds(pl.multiple_of((2 * near_x[k] + cc) * rows + ch * chunk, chunk), chunk)
            for k, ch in items
            for cc in (0, 1)
        ]

    def load_rows(ref, items):
        return jnp.concatenate([ref[r, :] for r in blocks_of(items)], axis=0)

    class Reduce:
        def __init__(self, n, lhs, weight):
            self.n, self.lhs, self.weight = n, lhs, weight
            self.sends, self.sib, self.got = [], {}, {}

        def project(self, *items):
            n = self.n
            cols = width // 4

            def body(j, carry):
                at = pl.ds(pl.multiple_of(j * cols, cols), cols)
                product = jnp.dot(
                    load_rows(self.lhs, items), self.weight[:, at], preferred_element_type=F32
                ).astype(BF16)
                for i, r in enumerate(blocks_of(items)):
                    part[r, at] = product[i * chunk : (i + 1) * chunk]
                return carry

            lax.fori_loop(0, 4, body, 0)
            for k, ch in items:
                i = 2 * k + ch
                start = pl.multiple_of((2 * near_x[k] + 1 - core) * rows + ch * chunk, chunk)
                s = copy(
                    part.at[pl.ds(start, chunk), :],
                    sib_in.at[n, k, pl.ds(ch * chunk, chunk)],
                    s_send.at[n, i],
                    s_recv.at[n, i],
                    sib,
                )
                s.start()
                self.sends.append(s)
                self.sib[k, ch] = s

        def paired(self, k, ch):
            self.sib[k, ch].wait_recv()

        def pre(self, k, ch, cols):
            at = pl.multiple_of((2 * near_x[k] + core) * rows + ch * chunk, chunk)
            r = slice(ch * chunk, (ch + 1) * chunk)
            return part[pl.ds(at, chunk), cols].astype(F32) + sib_in[self.n, k, r, cols].astype(F32)

        def ship(self, name, ch, slot_, value, cols, dst, device):
            n = self.n
            i = ch * 6 + ("pr", "pl", "dr", "dl", "sr", "sl").index(name)
            r = pl.ds(ch * chunk, chunk)
            stage[n, slot_, r, cols] = value.astype(BF16)
            s = copy(stage.at[n, slot_, r, cols], dst, r_send.at[n, i], r_recv.at[n, i], device)
            s.start()
            self.sends.append(s)
            self.got[name, ch] = s

        def passes(self, ch):
            self.paired(0, ch)
            n, r = self.n, pl.ds(ch * chunk, chunk)
            self.ship("pr", ch, 0, self.pre(0, ch, hi), hi, pass_in.at[n, 0, r], right)
            self.ship("pl", ch, 0, self.pre(0, ch, lo), lo, pass_in.at[n, 1, r], left)

        def direct_right(self, ch):
            self.paired(1, ch)
            dst = from_left.at[self.n, pl.ds(ch * chunk, chunk), lo]
            self.ship("dr", ch, 1, self.pre(1, ch, lo), lo, dst, right)

        def direct_left(self, ch):
            self.paired(2, ch)
            dst = from_right.at[self.n, pl.ds(ch * chunk, chunk), hi]
            self.ship("dl", ch, 2, self.pre(2, ch, hi), hi, dst, left)

        def sums(self, ch):
            n, r = self.n, pl.ds(ch * chunk, chunk)
            self.got["pr", ch].wait_recv()
            value = self.pre(1, ch, hi) + pass_in[n, 0, r].astype(F32)
            self.ship("sr", ch, 1, value, hi, from_left.at[n, r, hi], right)
            self.got["pl", ch].wait_recv()
            value = self.pre(2, ch, lo) + pass_in[n, 1, r].astype(F32)
            self.ship("sl", ch, 2, value, lo, from_right.at[n, r, lo], left)

        def arrive(self, ch):
            for name in ("dr", "dl", "sr", "sl"):
                self.got[name, ch].wait_recv()

        def total(self, at, count):
            n, r = self.n, pl.ds(at, count)
            base = pl.multiple_of((2 * x + core) * rows + at, count)
            return (
                (part[pl.ds(base, count), :].astype(F32) + sib_in[n, 3, r, :].astype(F32))
                + from_left[n, r, :].astype(F32)
                + from_right[n, r, :].astype(F32)
            )

        def drain(self):
            for s in self.sends:
                s.wait_send()

    one = Reduce(0, gp, w2)
    retain(0)
    y_whole(1)
    one.project((0, 0), (0, 1))
    poll()
    retain(1)
    one.passes(0)
    one.passes(1)
    one.project((1, 0), (1, 1))
    poll()
    retain(2)
    one.project((2, 0), (2, 1))
    one.direct_right(0)
    poll()
    retain(3)
    one.direct_left(0)
    one.sums(0)
    one.direct_right(1)
    one.direct_left(1)
    poll()
    one.project((3, 0), (3, 1))
    poll()
    one.sums(1)
    poll()
    one.paired(3, 0)
    one.paired(3, 1)
    poll()

    def mixed(i, carry):
        at = pl.multiple_of(i * 16, 16)
        after = tok[pl.ds(at, 16), :].astype(F32) + rms(one.total(at, 16)) * gains[1:2, :]
        am[pl.ds(at, 16), :] = after
        xw[pl.ds(pl.multiple_of(own + at, 16), 16), :] = (rms(after) * gains[2:3, :]).astype(BF16)
        return carry

    per = chunk // 16
    two = [gather(1, xw, 0, chunk), gather(2, xw, chunk, chunk)]
    one.arrive(0)
    lax.fori_loop(0, per, mixed, 0)
    two[0][0]()
    poll()
    poll()
    one.arrive(1)
    lax.fori_loop(per, 2 * per, mixed, 0)
    two[1][0]()
    poll()
    poll()
    one.drain()
    poll()
    two[0][1]()
    poll()
    poll()
    assert not polls

    def feed(*items):
        both = jnp.dot(load_rows(xw, items), w3[...], preferred_element_type=F32)
        hidden = (silu(both[:, 0:ff]) * both[:, ff:]).astype(BF16)
        for i, r in enumerate(blocks_of(items)):
            hid[r, :] = hidden[i * chunk : (i + 1) * chunk]

    last_one = Reduce(1, hid, w4)
    two[0][3]()
    two[1][3]()
    y_whole(2)
    feed((3, 0), (3, 1))
    two[0][4]()
    feed((1, 0), (2, 0))
    y_whole(3)
    last_one.project((1, 0), (2, 0))
    two[1][1]()
    last_one.direct_right(0)
    last_one.direct_left(0)
    two[0][2]()
    two[1][4]()
    feed((1, 1), (2, 1))
    last_one.project((1, 1), (2, 1))
    two[0][5]()
    feed((0, 0))
    last_one.project((0, 0))
    last_one.direct_right(1)
    last_one.direct_left(1)
    two[1][2]()
    last_one.passes(0)
    two[1][5]()
    feed((0, 1))
    last_one.project((0, 1))
    last_one.passes(1)
    last_one.project((3, 0), (3, 1))
    last_one.sums(0)
    last_one.sums(1)
    last_one.paired(3, 0)
    last_one.paired(3, 1)

    def last(i, carry):
        at = pl.multiple_of(i * 16, 16)
        r = pl.ds(at, 16)
        out[r, :] = (am[r, :] + rms(last_one.total(at, 16)) * gains[3:4, :]).astype(BF16)
        return carry

    last_one.arrive(0)
    lax.fori_loop(0, per, last, 0)
    last_one.arrive(1)
    lax.fori_loop(per, 2 * per, last, 0)
    drain1()
    two[0][6]()
    two[1][6]()
    last_one.drain()
    for a in range(4):
        y_drain(a)


def layer(nf, nx, tokens, gains, wq, wk, wv, ws, wo, wg, wu, wd):
    rows, width = tokens.shape
    seq = rows * 2 * nx
    qw, vw, ff = wq.shape[1], wv.shape[1], wg.shape[1]
    frequency = 10000.0 ** (-np.linspace(0.0, 1.0, qw // 2))
    within = np.arange(seq // 4, dtype=np.float64)[:, None] * frequency[None, :]
    starts = np.arange(4, dtype=np.float64)[:, None] * (seq // 4) * frequency[None, :]
    turn = jnp.asarray(np.stack([np.cos(within), np.sin(within)]).astype(np.float32))
    base = jnp.asarray(np.concatenate([np.cos(starts), np.sin(starts)]).astype(np.float32))
    heads = np.arange(2 * nx, dtype=np.float64)
    lam = -(4.0 / BLOCK) * (BLOCK / (32.0 * seq)) ** (heads / (H - 1))
    lam = jnp.asarray(np.repeat(lam[:, None], 128, axis=1).astype(np.float32))
    vmem = pl.BlockSpec(memory_space=pltpu.VMEM)
    hbm = pl.BlockSpec(memory_space=pl.ANY)
    dma = pltpu.SemaphoreType.DMA
    far = nf // 2
    half = width // 2
    n1 = 2 * qw + 2 * vw
    return pl.pallas_call(
        functools.partial(kernel, nf, nx),
        out_shape=jax.ShapeDtypeStruct((rows, width), BF16),
        in_specs=[vmem] * 3 + [hbm, vmem] + [hbm] * 8,
        out_specs=vmem,
        scratch_shapes=[
            pltpu.VMEM((width, n1), BF16),
            pltpu.VMEM((wo.shape[0], width), BF16),
            pltpu.VMEM((width, 2 * ff), BF16),
            pltpu.VMEM((wd.shape[0], width), BF16),
            pltpu.VMEM((seq, width), BF16),
            pltpu.VMEM((seq, width), BF16),
            pltpu.VMEM((seq, n1), F32),
            pltpu.VMEM((seq, qw), BF16),
            pltpu.VMEM((seq, qw), BF16),
            pltpu.VMEM((seq, vw), BF16),
            pltpu.VMEM((seq, vw), BF16),
            pltpu.VMEM((seq, ff), BF16),
            pltpu.VMEM((seq, width), BF16),
            pltpu.VMEM((2, nx, rows, width), BF16),
            pltpu.VMEM((2, 3, rows, width), BF16),
            pltpu.VMEM((2, 2, rows, half), BF16),
            pltpu.VMEM((2, rows, width), BF16),
            pltpu.VMEM((2, rows, width), BF16),
            pltpu.VMEM((rows, width), F32),
            pltpu.VMEM((2, seq // 4, qw // 2), F32),
            pltpu.VMEM((seq // 4, 2 * seq - seq // 4), F32),
            dma((10,)),
            dma((20,)),
            dma((20, far)),
            dma((10,)),
            dma((2 * far + 3,)),
            dma((3, 9)),
            dma((3, 9)),
            dma((2, 8)),
            dma((2, 8)),
            dma((2, 12)),
            dma((2, 12)),
        ],
        compiler_params=pltpu.CompilerParams(
            collective_id=0, has_side_effects=True, vmem_limit_bytes=66_000_000
        ),
    )(tokens, gains, lam, turn, base, wq, wk, wv, ws, wo, wg, wu, wd)


def solution(mesh):
    placed = (
        P(("grp", "fs", "tp"), None),
        P(),
        P("fs", "tp"),
        P("fs", "tp"),
        P("fs", "tp"),
        P("fs", "tp"),
        P("tp", "fs"),
        P("fs", "tp"),
        P("fs", "tp"),
        P("tp", "fs"),
    )
    nf, nt = mesh.shape["fs"], mesh.shape["tp"]
    assert mesh.shape["grp"] % 2 == 0 and nt == 8 and nf % 2 == 0
    return jax.shard_map(
        functools.partial(layer, nf, nt // 2),
        mesh=mesh,
        in_specs=placed,
        out_specs=P(("grp", "fs", "tp"), None),
        check_vma=False,
    )
```

```python
import functools

import jax
import jax.numpy as jnp
import numpy as np
from jax import lax
from jax.experimental import pallas as pl
from jax.experimental.pallas import tpu as pltpu
from jax.sharding import PartitionSpec as P

H = 8
BLOCK = 128
norm_epsilon = 1e-06
group_epsilon = 0.01
MESH = pl.DeviceIdType.MESH
F32 = jnp.float32
BF16 = jnp.bfloat16


def mod(a, n):
    return lax.rem(a + n, n)


def rms(matrix):
    return matrix * lax.rsqrt(jnp.mean(matrix * matrix, axis=-1, keepdims=True) + norm_epsilon)


def silu(v):
    return v / (1.0 + jnp.exp(-v))


def kernel(
    nf,
    nx,
    tok_hbm,
    gains_hbm,
    lam_hbm,
    turn_hbm,
    base_hbm,
    wq,
    wk,
    wv,
    ws,
    wo,
    wg,
    wu,
    wd,
    out,
    w1,
    w2,
    w3,
    w4,
    xn,
    xw,
    acc,
    qb,
    kb,
    vb,
    gp,
    hid,
    part,
    sib_in,
    stage,
    pass_in,
    from_left,
    from_right,
    am,
    turn,
    decay,
    tok,
    gains,
    lam_ref,
    base_ref,
    local_sem,
    z_send,
    z_recv,
    y_send,
    y_recv,
    g_send,
    g_recv,
    s_send,
    s_recv,
    r_send,
    r_recv,
):
    rows, width = tok.shape
    seq = xn.shape[0]
    half = width // 2
    quarter = seq // 4
    me = lax.axis_index("fs")
    tp = lax.axis_index("tp")
    group = lax.axis_index("grp")
    x = tp // 2
    core = lax.rem(tp, 2)
    plane = lax.rem(group, 2)
    up = {"fs": mod(me + 1, nf)}
    down = {"fs": mod(me - 1, nf)}
    pair = {"grp": group + 1 - 2 * plane}
    sib = {"tp": 2 * x + 1 - core}
    right = {"tp": 2 * mod(x + 1, nx) + core}
    left = {"tp": 2 * mod(x - 1, nx) + core}

    def copy(src, dst, send, recv, device):
        return pltpu.make_async_remote_copy(
            src_ref=src,
            dst_ref=dst,
            send_sem=send,
            recv_sem=recv,
            device_id=device,
            device_id_type=MESH,
        )

    kd = wq.shape[0]
    mine = pl.ds(pl.multiple_of(me * kd, kd), kd)
    mine_cols = pl.ds(pl.multiple_of(me * kd, kd), kd)
    qw, vw, ff = wq.shape[1], wv.shape[1], wg.shape[1]
    locals_ = [
        (wq, w1.at[mine, 0:qw]),
        (wk, w1.at[mine, qw : 2 * qw]),
        (wv, w1.at[mine, 2 * qw : 2 * qw + vw]),
        (ws, w1.at[mine, 2 * qw + vw : 2 * qw + 2 * vw]),
        (wo, w2.at[:, mine_cols]),
        (wg, w3.at[mine, 0:ff]),
        (wu, w3.at[mine, ff : 2 * ff]),
        (wd, w4.at[:, mine_cols]),
        (turn_hbm, turn),
        (lam_hbm, lam_ref),
        (base_hbm, base_ref),
        (tok_hbm, tok),
        (gains_hbm, gains),
    ]
    loads = [
        pltpu.make_async_copy(src, dst, local_sem.at[i]) for i, (src, dst) in enumerate(locals_)
    ]
    for load in loads[-2:] + loads[:-2]:
        load.start()

    barrier = pltpu.get_barrier_semaphore()
    for device in (up, down, pair, sib, right, left):
        pl.semaphore_signal(barrier, inc=1, device_id=device, device_id_type=MESH)

    own = pl.multiple_of(tp * rows, rows)

    def norm_in(i, carry):
        at = pl.multiple_of(i * 16, 16)
        value = rms(tok[pl.ds(at, 16), :].astype(F32)) * gains[0:1, :]
        xn[pl.ds(own + at, 16), :] = value.astype(BF16)
        return carry

    for load in loads[-2:]:
        load.wait()
    lax.fori_loop(0, rows // 16, norm_in, 0)
    pl.semaphore_wait(barrier, 6)

    def shared(a):
        return w2.shape[0] // 4 if a == 1 else w4.shape[0] // 3

    pieces = (4, 2, 4, 2)
    owns = (2, 1, 2, 1)

    def place(a, owner, piece, plane_, rows_half=None):
        ref = (w1, w2, w3, w4)[a]
        if a in (0, 2):
            w = ref.shape[1] // 3 // owns[a]
            start, count = owner * kd, kd
            if rows_half is not None:
                count = kd // 2
                start = start + rows_half * count
            r = pl.ds(pl.multiple_of(start, kd // 2), count)
            if piece < owns[a]:
                at = pl.multiple_of(plane_ * 2 * w * owns[a] + piece * w, 128)
            else:
                at = piece * w
            return ref.at[r, pl.ds(at, w)]
        t = shared(a)
        mid = ref.shape[0] - 2 * t
        r = pl.ds(pl.multiple_of(plane_ * (t + mid), 16), t) if piece == 0 else pl.ds(t, mid)
        return ref.at[r, pl.ds(pl.multiple_of(owner * kd, kd), kd)]

    half_streams = 2 * (pieces[0] + pieces[1])

    def z_index(a, d, piece):
        return 2 * sum(pieces[:a]) + d * pieces[a] + piece

    def y_index(a, d, piece):
        return 2 * sum(owns[:a]) + d * owns[a] + piece

    def owner_of(d, s):
        return mod(me - s, nf) if d == 0 else lax.rem(me + s, nf)

    far = nf // 2

    def z_copy(a, d, piece, s, rows_half=None):
        src = place(a, owner_of(d, s - 1), piece, plane, rows_half)
        k = z_index(a, d, piece)
        return copy(src, src, z_send.at[k], z_recv.at[k % half_streams, s - 1], up if d == 0 else down)

    def z_arrived(a, d, piece, s, rows_half=None):
        dst = place(a, owner_of(d, s), piece, plane, rows_half)
        k = z_index(a, d, piece)
        copy(dst, dst, z_send.at[k], z_recv.at[k % half_streams, s - 1], up if d == 0 else down).wait_recv()

    def y_sem(a, d, s):
        return y_recv.at[d * far + s - 1] if a == 0 else y_recv.at[2 * far + a - 1]

    def y_copy(a, d, piece, s, rows_half=None):
        src = place(a, owner_of(d, s), piece, plane, rows_half)
        return copy(src, src, y_send.at[y_index(a, d, piece)], y_sem(a, d, s), pair)

    def last_half(a, d):
        return d if a in (0, 2) else None

    def has_last(a, d):
        return a in (0, 2) or (a == 1 and d == 0) or (a == 3 and d == 1)

    def begin(a):
        for piece in range(pieces[a]):
            for d in (0, 1):
                z_copy(a, d, piece, 1).start()

    def forward(a, s, piece):
        for d in (0, 1):
            here = s < far or has_last(a, d)
            part_of = last_half(a, d) if s == far else None
            if here:
                z_arrived(a, d, piece, s, part_of)
                z_copy(a, d, piece, s, part_of).wait_send()
            if s < far - 1:
                z_copy(a, d, piece, s + 1).start()
            elif s == far - 1 and has_last(a, d):
                z_copy(a, d, piece, far, last_half(a, d)).start()
            if piece < owns[a]:
                if s > 1:
                    y_copy(a, d, piece, s - 1).wait_send()
                if here:
                    y_copy(a, d, piece, s, part_of).start()

    def slot(*items):
        for piece in range(4):
            for a, s in items:
                if piece < pieces[a]:
                    forward(a, s, piece)

    def y_step(s):
        w = w1.shape[1] // 3
        for d in (0, 1):
            count = kd if s < far else kd // 2
            start = owner_of(d, s) * kd + (0 if s < far else d * count)
            at = pl.multiple_of((1 - plane) * 2 * w, 128)
            dst = w1.at[pl.ds(pl.multiple_of(start, kd // 2), count), pl.ds(at, w)]
            copy(dst, dst, y_send.at[0], y_sem(0, d, s), pair).wait_recv()

    def y_whole(a):
        ref = (w1, w2, w3, w4)[a]
        n = (nf - 1) * kd
        if a == 2:
            w = ref.shape[1] // 3
            dst = ref.at[0:n, pl.ds(pl.multiple_of((1 - plane) * 2 * w, 128), w)]
        else:
            t = shared(a)
            dst = ref.at[pl.ds(pl.multiple_of((1 - plane) * (ref.shape[0] - t), 16), t), 0:n]
        copy(dst, dst, y_send.at[0], y_sem(a, 0, 1), pair).wait_recv()

    def y_drain(a):
        for piece in range(owns[a]):
            for d in (0, 1):
                if has_last(a, d):
                    y_copy(a, d, piece, far, last_half(a, d)).wait_send()

    def gather(n, ref, at, count):
        at_left, at_right, at_far = mod(x - 1, nx), mod(x + 1, nx), mod(x + 2, nx)
        lo, hi = pl.ds(0, half), pl.ds(half, half)
        every = pl.ds(0, width)

        def whole(xx, cc, cols=every):
            return ref.at[pl.ds(pl.multiple_of((2 * xx + cc) * rows + at, count), count), cols]

        def send(k, xx, cols, device):
            src = whole(xx, core, cols)
            return copy(src, src, g_send.at[n // 2, k], g_recv.at[n // 2, k], device)

        def arrived(k, xx, cc, cols):
            dst = whole(xx, cc, cols)
            copy(dst, dst, g_send.at[n // 2, k], g_recv.at[n // 2, k], sib).wait_recv()

        sends = []

        def go(*args):
            s = send(*args)
            s.start()
            sends.append(s)

        def first():
            go(1, x, every, right)
            go(2, x, every, left)
            go(0, x, every, sib)

        def second():
            arrived(1, at_left, core, every)
            go(3, at_left, lo, right)
            go(4, at_left, every, sib)
            arrived(2, at_right, core, every)
            go(5, at_right, hi, left)
            go(6, at_right, every, sib)

        def third_():
            arrived(3, at_far, core, lo)
            go(7, at_far, lo, sib)
            arrived(5, at_far, core, hi)
            go(8, at_far, hi, sib)

        def own_chip():
            arrived(0, x, 1 - core, every)

        def near():
            arrived(4, at_left, 1 - core, every)
            arrived(6, at_right, 1 - core, every)

        def rest():
            arrived(7, at_far, 1 - core, lo)
            arrived(8, at_far, 1 - core, hi)

        def drain():
            for s in sends:
                s.wait_send()

        return first, second, third_, own_chip, near, rest, drain

    for load in loads[:4]:
        load.wait()
    begin(0)
    first, second, third_, own_chip, near, rest, drain1 = gather(0, xn, 0, rows)
    first()

    for load in loads[4:-2]:
        load.wait()

    lam = lam_ref[pl.ds(tp, 1), 0:1]
    dn = lax.broadcasted_iota(jnp.int32, decay.shape, 0) + (seq - quarter)
    dm = lax.broadcasted_iota(jnp.int32, decay.shape, 1)
    dist = (dn - dm).astype(F32)
    decay[...] = jnp.where(dist >= 0.0, jnp.exp(lam * jnp.maximum(dist, 0.0)), 0.0)

    def k_slice(owner):
        return pl.ds(pl.multiple_of(owner * kd, kd), kd)

    def tiled(tiles, body):
        n = acc.shape[1] // 2

        def step(i, carry):
            r = pl.ds(pl.multiple_of(i // 2 * quarter, quarter), quarter)
            body(r, pl.ds(pl.multiple_of(lax.rem(i, 2) * n, n), n))
            return carry

        lax.fori_loop(2 * tiles[0], 2 * tiles[1], step, 0)

    def add_own(tiles):
        def body(r, c):
            acc[r, c] = jnp.dot(
                xn[r, k_slice(me)], w1[k_slice(me), c], preferred_element_type=F32
            )

        tiled(tiles, body)

    def add_two(s, tiles):
        a, b = k_slice(owner_of(0, s)), k_slice(owner_of(1, s))

        def body(r, c):
            acc[r, c] = (
                acc[r, c]
                + jnp.dot(xn[r, a], w1[a, c], preferred_element_type=F32)
                + jnp.dot(xn[r, b], w1[b, c], preferred_element_type=F32)
            )

        tiled(tiles, body)

    def slot_and_add(s, adds):
        for piece in range(4):
            forward(0, s, piece)
            if piece < 3:
                for waits, add, tiles in adds[piece]:
                    if waits:
                        y_step(waits)
                    add(tiles)
        forward(1, s, 0)
        forward(1, s, 1)

    order = (((2, 0), (3, 0)), ((2, 1),), ((2, 2), (3, 1)), ((2, 3),))
    polls = [(s, group) for s in range(1, far + 1) for group in order]

    def poll(count=1):
        for _ in range(count):
            s, group = polls.pop(0)
            for a, piece in group:
                forward(a, s, piece)

    def begin_polled():
        for group in order:
            for a, piece in group:
                for d in (0, 1):
                    z_copy(a, d, piece, 1).start()

    def two_of(s, tiles, wait=True):
        return s if wait else 0, functools.partial(add_two, s), tiles

    begin(1)
    slot((0, 1))
    forward(1, 1, 0)
    forward(1, 1, 1)
    second()
    slot((0, 2))
    forward(1, 2, 0)
    forward(1, 2, 1)
    own_chip()
    third_()
    forward(0, 3, 0)
    forward(0, 3, 1)
    near()
    rest()
    forward(0, 3, 2)
    forward(0, 3, 3)
    forward(1, 3, 0)
    forward(1, 3, 1)
    slot_and_add(4, ([(0, add_own, (0, 4))], [two_of(1, (0, 4))], [two_of(2, (0, 4))]))
    slot_and_add(5, ([two_of(3, (0, 4))], [], [two_of(4, (0, 4))]))
    for s in range(6, far):
        slot_and_add(s, ([], [], [two_of(s - 1, (0, 4))]))
    begin_polled()
    slot_and_add(far, ([], [two_of(far - 1, (0, 2))], [two_of(far - 1, (2, 4), False)]))
    y_step(far)
    far_slice = k_slice(owner_of(0, far))

    key_scale = float(qw) ** -0.5
    hq = qw // 2

    def finish(i, carry):
        r = pl.ds(pl.multiple_of(i * quarter, quarter), quarter)
        total = acc[r, :] + jnp.dot(xn[r, far_slice], w1[far_slice, :], preferred_element_type=F32)
        cb, sb = base_ref[pl.ds(i, 1), :], base_ref[pl.ds(i + 4, 1), :]
        c = cb * turn[0] - sb * turn[1]
        s = sb * turn[0] + cb * turn[1]
        for ref, at, scale in ((qb, 0, None), (kb, qw, key_scale)):
            a, b = total[:, at : at + hq], total[:, at + hq : at + qw]
            first_half = a * c - b * s
            second_half = a * s + b * c
            if scale is not None:
                first_half, second_half = first_half * scale, second_half * scale
            ref[r, 0:hq] = first_half.astype(BF16)
            ref[r, hq:qw] = second_half.astype(BF16)
        vb[r, :] = total[:, 2 * qw : 2 * qw + vw].astype(BF16)
        acc[r, 2 * qw + vw :] = total[:, 2 * qw + vw :]
        return carry

    lax.fori_loop(0, 4, finish, 0)
    poll(2)

    near_x = (mod(x + 2, nx), mod(x + 1, nx), mod(x - 1, nx), x)

    def retain(k):
        i = near_x[k]
        r = pl.ds(pl.multiple_of(i * quarter, quarter), quarter)
        seen = pl.ds(pl.multiple_of((nx - 1 - i) * quarter, quarter), seq)
        scores = lax.dot_general(
            qb[r, :], kb[...], (((1,), (1,)), ((), ())), preferred_element_type=F32
        )
        weighted = (scores * decay[:, seen]).astype(BF16)
        retained = jnp.dot(weighted, vb[...], preferred_element_type=F32)
        centred = retained - jnp.mean(retained, axis=-1, keepdims=True)
        normalized = centred * lax.rsqrt(
            jnp.mean(centred * centred, axis=-1, keepdims=True) + group_epsilon
        )
        gp[r, :] = (silu(acc[r, 2 * qw + vw :]) * normalized).astype(BF16)

    lo, hi = slice(0, half), slice(half, width)
    chunk = rows // 2

    def blocks_of(items):
        return [
            pl.ds(pl.multiple_of((2 * near_x[k] + cc) * rows + ch * chunk, chunk), chunk)
            for k, ch in items
            for cc in (0, 1)
        ]

    def load_rows(ref, items):
        return jnp.concatenate([ref[r, :] for r in blocks_of(items)], axis=0)

    class Reduce:
        def __init__(self, n, lhs, weight):
            self.n, self.lhs, self.weight = n, lhs, weight
            self.sends, self.sib, self.got = [], {}, {}

        def project(self, *items):
            n = self.n
            cols = width // 4

            def body(j, carry):
                at = pl.ds(pl.multiple_of(j * cols, cols), cols)
                product = jnp.dot(
                    load_rows(self.lhs, items), self.weight[:, at], preferred_element_type=F32
                ).astype(BF16)
                for i, r in enumerate(blocks_of(items)):
                    part[r, at] = product[i * chunk : (i + 1) * chunk]
                return carry

            lax.fori_loop(0, 4, body, 0)
            for k, ch in items:
                i = 2 * k + ch
                start = pl.multiple_of((2 * near_x[k] + 1 - core) * rows + ch * chunk, chunk)
                s = copy(
                    part.at[pl.ds(start, chunk), :],
                    sib_in.at[n, k, pl.ds(ch * chunk, chunk)],
                    s_send.at[i],
                    s_recv.at[i],
                    sib,
                )
                s.start()
                self.sends.append(s)
                self.sib[k, ch] = s

        def paired(self, k, ch):
            self.sib[k, ch].wait_recv()

        def pre(self, k, ch, cols):
            at = pl.multiple_of((2 * near_x[k] + core) * rows + ch * chunk, chunk)
            r = slice(ch * chunk, (ch + 1) * chunk)
            return part[pl.ds(at, chunk), cols].astype(F32) + sib_in[self.n, k, r, cols].astype(F32)

        def ship(self, name, ch, slot_, value, cols, dst, device):
            n = self.n
            i = ch * 6 + ("pr", "pl", "dr", "dl", "sr", "sl").index(name)
            r = pl.ds(ch * chunk, chunk)
            stage[n, slot_, r, cols] = value.astype(BF16)
            s = copy(stage.at[n, slot_, r, cols], dst, r_send.at[i], r_recv.at[i], device)
            s.start()
            self.sends.append(s)
            self.got[name, ch] = s

        def passes(self, ch):
            self.paired(0, ch)
            n, r = self.n, pl.ds(ch * chunk, chunk)
            self.ship("pr", ch, 0, self.pre(0, ch, hi), hi, pass_in.at[n, 0, r], right)
            self.ship("pl", ch, 0, self.pre(0, ch, lo), lo, pass_in.at[n, 1, r], left)

        def direct_right(self, ch):
            self.paired(1, ch)
            dst = from_left.at[self.n, pl.ds(ch * chunk, chunk), lo]
            self.ship("dr", ch, 1, self.pre(1, ch, lo), lo, dst, right)

        def direct_left(self, ch):
            self.paired(2, ch)
            dst = from_right.at[self.n, pl.ds(ch * chunk, chunk), hi]
            self.ship("dl", ch, 2, self.pre(2, ch, hi), hi, dst, left)

        def sums(self, ch):
            n, r = self.n, pl.ds(ch * chunk, chunk)
            self.got["pr", ch].wait_recv()
            value = self.pre(1, ch, hi) + pass_in[n, 0, r].astype(F32)
            self.ship("sr", ch, 1, value, hi, from_left.at[n, r, hi], right)
            self.got["pl", ch].wait_recv()
            value = self.pre(2, ch, lo) + pass_in[n, 1, r].astype(F32)
            self.ship("sl", ch, 2, value, lo, from_right.at[n, r, lo], left)

        def arrive(self, ch):
            for name in ("dr", "dl", "sr", "sl"):
                self.got[name, ch].wait_recv()

        def total(self, at, count):
            n, r = self.n, pl.ds(at, count)
            base = pl.multiple_of((2 * x + core) * rows + at, count)
            return (
                (part[pl.ds(base, count), :].astype(F32) + sib_in[n, 3, r, :].astype(F32))
                + from_left[n, r, :].astype(F32)
                + from_right[n, r, :].astype(F32)
            )

        def drain(self):
            for s in self.sends:
                s.wait_send()

    one = Reduce(0, gp, w2)
    retain(0)
    y_whole(1)
    one.project((0, 0), (0, 1))
    poll()
    one.passes(0)
    one.passes(1)
    retain(1)
    poll(2)
    one.project((1, 0), (1, 1))
    poll(2)
    retain(2)
    poll()
    one.project((2, 0), (2, 1))
    one.direct_right(0)
    poll()
    retain(3)
    one.direct_left(0)
    poll()
    one.sums(0)
    one.direct_right(1)
    one.direct_left(1)
    poll(2)
    one.project((3, 0), (3, 1))
    poll()
    one.sums(1)
    poll(3)
    one.paired(3, 0)
    one.paired(3, 1)
    poll(2)
    drain1()

    def mixed(i, carry):
        at = pl.multiple_of(i * 16, 16)
        after = tok[pl.ds(at, 16), :].astype(F32) + rms(one.total(at, 16)) * gains[1:2, :]
        am[pl.ds(at, 16), :] = after
        xw[pl.ds(pl.multiple_of(own + at, 16), 16), :] = (rms(after) * gains[2:3, :]).astype(BF16)
        return carry

    per = chunk // 16
    two = [gather(1, xw, 0, chunk), gather(2, xw, chunk, chunk)]
    one.arrive(0)
    lax.fori_loop(0, per, mixed, 0)
    two[0][0]()
    poll(4)
    one.arrive(1)
    lax.fori_loop(per, 2 * per, mixed, 0)
    two[1][0]()
    one.drain()
    poll(5)
    two[0][1]()
    poll(5)
    assert not polls

    def feed(*items):
        both = jnp.dot(load_rows(xw, items), w3[...], preferred_element_type=F32)
        hidden = (silu(both[:, 0:ff]) * both[:, ff:]).astype(BF16)
        for i, r in enumerate(blocks_of(items)):
            hid[r, :] = hidden[i * chunk : (i + 1) * chunk]

    last_one = Reduce(1, hid, w4)
    two[1][1]()
    y_whole(2)
    two[0][4]()
    feed((1, 0), (2, 0))
    y_whole(3)
    last_one.project((1, 0), (2, 0))
    two[0][2]()
    two[1][4]()
    feed((1, 1), (2, 1))
    last_one.direct_right(0)
    last_one.direct_left(0)
    last_one.project((1, 1), (2, 1))
    two[1][2]()
    two[0][5]()
    feed((0, 0))
    last_one.project((0, 0))
    last_one.direct_right(1)
    last_one.direct_left(1)
    two[1][5]()
    feed((0, 1))
    last_one.passes(0)
    last_one.project((0, 1))
    two[0][3]()
    two[1][3]()
    feed((3, 0), (3, 1))
    last_one.passes(1)
    last_one.project((3, 0), (3, 1))
    last_one.sums(0)
    last_one.sums(1)
    last_one.paired(3, 0)
    last_one.paired(3, 1)

    def last(i, carry):
        at = pl.multiple_of(i * 16, 16)
        r = pl.ds(at, 16)
        out[r, :] = (am[r, :] + rms(last_one.total(at, 16)) * gains[3:4, :]).astype(BF16)
        return carry

    last_one.arrive(0)
    lax.fori_loop(0, per, last, 0)
    last_one.arrive(1)
    lax.fori_loop(per, 2 * per, last, 0)
    two[0][6]()
    two[1][6]()
    last_one.drain()
    for a in range(4):
        y_drain(a)


def layer(nf, nx, tokens, gains, wq, wk, wv, ws, wo, wg, wu, wd):
    rows, width = tokens.shape
    seq = rows * 2 * nx
    qw, vw, ff = wq.shape[1], wv.shape[1], wg.shape[1]
    frequency = 10000.0 ** (-np.linspace(0.0, 1.0, qw // 2))
    within = np.arange(seq // 4, dtype=np.float64)[:, None] * frequency[None, :]
    starts = np.arange(4, dtype=np.float64)[:, None] * (seq // 4) * frequency[None, :]
    turn = jnp.asarray(np.stack([np.cos(within), np.sin(within)]).astype(np.float32))
    base = jnp.asarray(np.concatenate([np.cos(starts), np.sin(starts)]).astype(np.float32))
    heads = np.arange(2 * nx, dtype=np.float64)
    lam = -(4.0 / BLOCK) * (BLOCK / (32.0 * seq)) ** (heads / (H - 1))
    lam = jnp.asarray(np.repeat(lam[:, None], 128, axis=1).astype(np.float32))
    vmem = pl.BlockSpec(memory_space=pltpu.VMEM)
    hbm = pl.BlockSpec(memory_space=pl.ANY)
    dma = pltpu.SemaphoreType.DMA
    far = nf // 2
    half = width // 2
    n1 = 2 * qw + 2 * vw
    return pl.pallas_call(
        functools.partial(kernel, nf, nx),
        out_shape=jax.ShapeDtypeStruct((rows, width), BF16),
        in_specs=[hbm] * 13,
        out_specs=vmem,
        scratch_shapes=[
            pltpu.VMEM((width, n1), BF16),
            pltpu.VMEM((wo.shape[0], width), BF16),
            pltpu.VMEM((width, 2 * ff), BF16),
            pltpu.VMEM((wd.shape[0], width), BF16),
            pltpu.VMEM((seq, width), BF16),
            pltpu.VMEM((seq, width), BF16),
            pltpu.VMEM((seq, n1), F32),
            pltpu.VMEM((seq, qw), BF16),
            pltpu.VMEM((seq, qw), BF16),
            pltpu.VMEM((seq, vw), BF16),
            pltpu.VMEM((seq, vw), BF16),
            pltpu.VMEM((seq, ff), BF16),
            pltpu.VMEM((seq, width), BF16),
            pltpu.VMEM((2, nx, rows, width), BF16),
            pltpu.VMEM((2, 3, rows, width), BF16),
            pltpu.VMEM((2, 2, rows, half), BF16),
            pltpu.VMEM((2, rows, width), BF16),
            pltpu.VMEM((2, rows, width), BF16),
            pltpu.VMEM((rows, width), F32),
            pltpu.VMEM((2, seq // 4, qw // 2), F32),
            pltpu.VMEM((seq // 4, 2 * seq - seq // 4), F32),
            pltpu.VMEM(tokens.shape, BF16),
            pltpu.VMEM(gains.shape, F32),
            pltpu.VMEM(lam.shape, F32),
            pltpu.VMEM(base.shape, F32),
            dma((13,)),
            dma((24,)),
            dma((12, far)),
            dma((12,)),
            dma((2 * far + 3,)),
            dma((2, 9)),
            dma((2, 9)),
            dma((8,)),
            dma((8,)),
            dma((12,)),
            dma((12,)),
        ],
        compiler_params=pltpu.CompilerParams(
            collective_id=0, has_side_effects=True, vmem_limit_bytes=66_000_000
        ),
    )(tokens, gains, lam, turn, base, wq, wk, wv, ws, wo, wg, wu, wd)


def solution(mesh):
    placed = (
        P(("grp", "fs", "tp"), None),
        P(),
        P("fs", "tp"),
        P("fs", "tp"),
        P("fs", "tp"),
        P("fs", "tp"),
        P("tp", "fs"),
        P("fs", "tp"),
        P("fs", "tp"),
        P("tp", "fs"),
    )
    nf, nt = mesh.shape["fs"], mesh.shape["tp"]
    assert mesh.shape["grp"] % 2 == 0 and nt == 8 and nf % 2 == 0
    return jax.shard_map(
        functools.partial(layer, nf, nt // 2),
        mesh=mesh,
        in_specs=placed,
        out_specs=P(("grp", "fs", "tp"), None),
        check_vma=False,
    )
```

```python
import functools

import jax
import jax.numpy as jnp
import numpy as np
from jax import lax
from jax.experimental import pallas as pl
from jax.experimental.pallas import tpu as pltpu
from jax.sharding import PartitionSpec as P

H = 8
BLOCK = 128
norm_epsilon = 1e-06
group_epsilon = 0.01
MESH = pl.DeviceIdType.MESH
F32 = jnp.float32
BF16 = jnp.bfloat16


def mod(a, n):
    return lax.rem(a + n, n)


def rms(matrix):
    return matrix * lax.rsqrt(jnp.mean(matrix * matrix, axis=-1, keepdims=True) + norm_epsilon)


def silu(v):
    return v / (1.0 + jnp.exp(-v))


def kernel(
    nf,
    nx,
    tok_hbm,
    gains_hbm,
    lam_hbm,
    turn_hbm,
    base_hbm,
    wq,
    wk,
    wv,
    ws,
    wo,
    wg,
    wu,
    wd,
    out,
    w1,
    w2,
    w3,
    w4,
    xn,
    xw,
    acc,
    qb,
    kb,
    vb,
    gp,
    hid,
    part,
    sib_in,
    stage,
    pass_in,
    from_left,
    from_right,
    am,
    turn,
    decay,
    tok,
    gains,
    lam_ref,
    base_ref,
    local_sem,
    z_send,
    z_recv,
    y_send,
    y_recv,
    g_send,
    g_recv,
    s_send,
    s_recv,
    r_send,
    r_recv,
):
    rows, width = tok.shape
    seq = xn.shape[0]
    half = width // 2
    quarter = seq // 4
    me = lax.axis_index("fs")
    tp = lax.axis_index("tp")
    group = lax.axis_index("grp")
    x = tp // 2
    core = lax.rem(tp, 2)
    plane = lax.rem(group, 2)
    up = {"fs": mod(me + 1, nf)}
    down = {"fs": mod(me - 1, nf)}
    pair = {"grp": group + 1 - 2 * plane}
    sib = {"tp": 2 * x + 1 - core}
    right = {"tp": 2 * mod(x + 1, nx) + core}
    left = {"tp": 2 * mod(x - 1, nx) + core}

    def copy(src, dst, send, recv, device):
        return pltpu.make_async_remote_copy(
            src_ref=src,
            dst_ref=dst,
            send_sem=send,
            recv_sem=recv,
            device_id=device,
            device_id_type=MESH,
        )

    kd = wq.shape[0]
    mine = pl.ds(pl.multiple_of(me * kd, kd), kd)
    mine_cols = pl.ds(pl.multiple_of(me * kd, kd), kd)
    qw, vw, ff = wq.shape[1], wv.shape[1], wg.shape[1]
    locals_ = [
        (wq, w1.at[mine, 0:qw]),
        (wk, w1.at[mine, qw : 2 * qw]),
        (wv, w1.at[mine, 2 * qw : 2 * qw + vw]),
        (ws, w1.at[mine, 2 * qw + vw : 2 * qw + 2 * vw]),
        (wo, w2.at[:, mine_cols]),
        (wg, w3.at[mine, 0:ff]),
        (wu, w3.at[mine, ff : 2 * ff]),
        (wd, w4.at[:, mine_cols]),
        (turn_hbm, turn),
        (lam_hbm, lam_ref),
        (base_hbm, base_ref),
        (tok_hbm, tok),
        (gains_hbm, gains),
    ]
    loads = [
        pltpu.make_async_copy(src, dst, local_sem.at[i]) for i, (src, dst) in enumerate(locals_)
    ]
    for load in loads[-2:] + loads[:-2]:
        load.start()

    barrier = pltpu.get_barrier_semaphore()
    for device in (up, down, pair, sib, right, left):
        pl.semaphore_signal(barrier, inc=1, device_id=device, device_id_type=MESH)

    own = pl.multiple_of(tp * rows, rows)

    def norm_in(i, carry):
        at = pl.multiple_of(i * 16, 16)
        value = rms(tok[pl.ds(at, 16), :].astype(F32)) * gains[0:1, :]
        xn[pl.ds(own + at, 16), :] = value.astype(BF16)
        return carry

    for load in loads[-2:]:
        load.wait()
    lax.fori_loop(0, rows // 16, norm_in, 0)
    pl.semaphore_wait(barrier, 6)

    def shared(a):
        return w2.shape[0] // 4 if a == 1 else w4.shape[0] // 3

    pieces = (4, 2, 4, 2)
    owns = (2, 1, 2, 1)

    def place(a, owner, piece, plane_, rows_half=None):
        ref = (w1, w2, w3, w4)[a]
        if a in (0, 2):
            w = ref.shape[1] // 3 // owns[a]
            start, count = owner * kd, kd
            if rows_half is not None:
                count = kd // 2
                start = start + rows_half * count
            r = pl.ds(pl.multiple_of(start, kd // 2), count)
            if piece < owns[a]:
                at = pl.multiple_of(plane_ * 2 * w * owns[a] + piece * w, 128)
            else:
                at = piece * w
            return ref.at[r, pl.ds(at, w)]
        t = shared(a)
        mid = ref.shape[0] - 2 * t
        r = pl.ds(pl.multiple_of(plane_ * (t + mid), 16), t) if piece == 0 else pl.ds(t, mid)
        return ref.at[r, pl.ds(pl.multiple_of(owner * kd, kd), kd)]

    half_streams = 2 * (pieces[0] + pieces[1])

    def z_index(a, d, piece):
        return 2 * sum(pieces[:a]) + d * pieces[a] + piece

    def y_index(a, d, piece):
        return 2 * sum(owns[:a]) + d * owns[a] + piece

    def owner_of(d, s):
        return mod(me - s, nf) if d == 0 else lax.rem(me + s, nf)

    far = nf // 2

    def z_copy(a, d, piece, s, rows_half=None):
        src = place(a, owner_of(d, s - 1), piece, plane, rows_half)
        k = z_index(a, d, piece)
        return copy(src, src, z_send.at[k], z_recv.at[k % half_streams, s - 1], up if d == 0 else down)

    def z_arrived(a, d, piece, s, rows_half=None):
        dst = place(a, owner_of(d, s), piece, plane, rows_half)
        k = z_index(a, d, piece)
        copy(dst, dst, z_send.at[k], z_recv.at[k % half_streams, s - 1], up if d == 0 else down).wait_recv()

    def y_sem(a, d, s):
        return y_recv.at[d * far + s - 1] if a == 0 else y_recv.at[2 * far + a - 1]

    def y_copy(a, d, piece, s, rows_half=None):
        src = place(a, owner_of(d, s), piece, plane, rows_half)
        return copy(src, src, y_send.at[y_index(a, d, piece)], y_sem(a, d, s), pair)

    def last_half(a, d):
        return d if a in (0, 2) else None

    def has_last(a, d):
        return a in (0, 2) or (a == 1 and d == 0) or (a == 3 and d == 1)

    def begin(a):
        for piece in range(pieces[a]):
            for d in (0, 1):
                z_copy(a, d, piece, 1).start()

    def forward(a, s, piece):
        for d in (0, 1):
            here = s < far or has_last(a, d)
            part_of = last_half(a, d) if s == far else None
            if here:
                z_arrived(a, d, piece, s, part_of)
                z_copy(a, d, piece, s, part_of).wait_send()
            if s < far - 1:
                z_copy(a, d, piece, s + 1).start()
            elif s == far - 1 and has_last(a, d):
                z_copy(a, d, piece, far, last_half(a, d)).start()
            if piece < owns[a]:
                if s > 1:
                    y_copy(a, d, piece, s - 1).wait_send()
                if here:
                    y_copy(a, d, piece, s, part_of).start()

    def slot(*items):
        for piece in range(4):
            for a, s in items:
                if piece < pieces[a]:
                    forward(a, s, piece)

    def y_step(s):
        w = w1.shape[1] // 3
        for d in (0, 1):
            count = kd if s < far else kd // 2
            start = owner_of(d, s) * kd + (0 if s < far else d * count)
            at = pl.multiple_of((1 - plane) * 2 * w, 128)
            dst = w1.at[pl.ds(pl.multiple_of(start, kd // 2), count), pl.ds(at, w)]
            copy(dst, dst, y_send.at[0], y_sem(0, d, s), pair).wait_recv()

    def y_whole(a):
        ref = (w1, w2, w3, w4)[a]
        n = (nf - 1) * kd
        if a == 2:
            w = ref.shape[1] // 3
            dst = ref.at[0:n, pl.ds(pl.multiple_of((1 - plane) * 2 * w, 128), w)]
        else:
            t = shared(a)
            dst = ref.at[pl.ds(pl.multiple_of((1 - plane) * (ref.shape[0] - t), 16), t), 0:n]
        copy(dst, dst, y_send.at[0], y_sem(a, 0, 1), pair).wait_recv()

    def y_drain(a):
        for piece in range(owns[a]):
            for d in (0, 1):
                if has_last(a, d):
                    y_copy(a, d, piece, far, last_half(a, d)).wait_send()

    def gather(n, ref, at, count):
        at_left, at_right, at_far = mod(x - 1, nx), mod(x + 1, nx), mod(x + 2, nx)
        lo, hi = pl.ds(0, half), pl.ds(half, half)
        every = pl.ds(0, width)

        def whole(xx, cc, cols=every):
            return ref.at[pl.ds(pl.multiple_of((2 * xx + cc) * rows + at, count), count), cols]

        def send(k, xx, cols, device):
            src = whole(xx, core, cols)
            return copy(src, src, g_send.at[n // 2, k], g_recv.at[n // 2, k], device)

        def arrived(k, xx, cc, cols):
            dst = whole(xx, cc, cols)
            copy(dst, dst, g_send.at[n // 2, k], g_recv.at[n // 2, k], sib).wait_recv()

        sends = []

        def go(*args):
            s = send(*args)
            s.start()
            sends.append(s)

        def first():
            go(1, x, every, right)
            go(2, x, every, left)
            go(0, x, every, sib)

        def second():
            arrived(1, at_left, core, every)
            go(3, at_left, lo, right)
            go(4, at_left, every, sib)
            arrived(2, at_right, core, every)
            go(5, at_right, hi, left)
            go(6, at_right, every, sib)

        def third_():
            arrived(3, at_far, core, lo)
            go(7, at_far, lo, sib)
            arrived(5, at_far, core, hi)
            go(8, at_far, hi, sib)

        def own_chip():
            arrived(0, x, 1 - core, every)

        def near():
            arrived(4, at_left, 1 - core, every)
            arrived(6, at_right, 1 - core, every)

        def rest():
            arrived(7, at_far, 1 - core, lo)
            arrived(8, at_far, 1 - core, hi)

        def drain():
            for s in sends:
                s.wait_send()

        return first, second, third_, own_chip, near, rest, drain

    for load in loads[:4]:
        load.wait()
    begin(0)
    first, second, third_, own_chip, near, rest, drain1 = gather(0, xn, 0, rows)
    first()

    for load in loads[4:-2]:
        load.wait()

    lam = lam_ref[pl.ds(tp, 1), 0:1]
    dn = lax.broadcasted_iota(jnp.int32, decay.shape, 0) + (seq - quarter)
    dm = lax.broadcasted_iota(jnp.int32, decay.shape, 1)
    dist = (dn - dm).astype(F32)
    decay[...] = jnp.where(dist >= 0.0, jnp.exp(lam * jnp.maximum(dist, 0.0)), 0.0)

    def k_slice(owner):
        return pl.ds(pl.multiple_of(owner * kd, kd), kd)

    def tiled(tiles, body):
        n = acc.shape[1] // 2

        def step(i, carry):
            r = pl.ds(pl.multiple_of(i // 2 * quarter, quarter), quarter)
            body(r, pl.ds(pl.multiple_of(lax.rem(i, 2) * n, n), n))
            return carry

        lax.fori_loop(2 * tiles[0], 2 * tiles[1], step, 0)

    def add_own(tiles):
        def body(r, c):
            acc[r, c] = jnp.dot(
                xn[r, k_slice(me)], w1[k_slice(me), c], preferred_element_type=F32
            )

        tiled(tiles, body)

    def add_two(s, tiles):
        a, b = k_slice(owner_of(0, s)), k_slice(owner_of(1, s))

        def body(r, c):
            acc[r, c] = (
                acc[r, c]
                + jnp.dot(xn[r, a], w1[a, c], preferred_element_type=F32)
                + jnp.dot(xn[r, b], w1[b, c], preferred_element_type=F32)
            )

        tiled(tiles, body)

    def slot_and_add(s, adds):
        for piece in range(4):
            forward(0, s, piece)
            if piece < 3:
                for waits, add, tiles in adds[piece]:
                    if waits:
                        y_step(waits)
                    add(tiles)
        forward(1, s, 0)
        forward(1, s, 1)

    order = (((2, 0), (3, 0)), ((2, 1),), ((2, 2), (3, 1)), ((2, 3),))
    polls = [(s, group) for s in range(1, far + 1) for group in order]

    def pass_on(s, group):
        for a, piece in group:
            forward(a, s, piece)

    def poll(count=1):
        for _ in range(count):
            pass_on(*polls.pop(0))

    def begin_polled():
        for group in order:
            for a, piece in group:
                for d in (0, 1):
                    z_copy(a, d, piece, 1).start()

    def two_of(s, tiles, wait=True):
        return s if wait else 0, functools.partial(add_two, s), tiles

    begin(1)
    slot((0, 1))
    forward(1, 1, 0)
    forward(1, 1, 1)
    second()
    slot((0, 2))
    forward(1, 2, 0)
    forward(1, 2, 1)
    own_chip()
    third_()
    forward(0, 3, 0)
    forward(0, 3, 1)
    near()
    rest()
    forward(0, 3, 2)
    forward(0, 3, 3)
    forward(1, 3, 0)
    forward(1, 3, 1)
    slot_and_add(4, ([(0, add_own, (0, 4))], [two_of(1, (0, 4))], [two_of(2, (0, 4))]))
    slot_and_add(5, ([two_of(3, (0, 4))], [], [two_of(4, (0, 4))]))
    for s in range(6, far):
        slot_and_add(s, ([], [], [two_of(s - 1, (0, 4))]))
    begin_polled()
    slot_and_add(far, ([], [two_of(far - 1, (0, 2))], [two_of(far - 1, (2, 4), False)]))
    y_step(far)
    far_slice = k_slice(owner_of(0, far))

    key_scale = float(qw) ** -0.5
    hq = qw // 2

    def finish(i, carry):
        r = pl.ds(pl.multiple_of(i * quarter, quarter), quarter)
        total = acc[r, :] + jnp.dot(xn[r, far_slice], w1[far_slice, :], preferred_element_type=F32)
        cb, sb = base_ref[pl.ds(i, 1), :], base_ref[pl.ds(i + 4, 1), :]
        c = cb * turn[0] - sb * turn[1]
        s = sb * turn[0] + cb * turn[1]
        for ref, at, scale in ((qb, 0, None), (kb, qw, key_scale)):
            a, b = total[:, at : at + hq], total[:, at + hq : at + qw]
            first_half = a * c - b * s
            second_half = a * s + b * c
            if scale is not None:
                first_half, second_half = first_half * scale, second_half * scale
            ref[r, 0:hq] = first_half.astype(BF16)
            ref[r, hq:qw] = second_half.astype(BF16)
        vb[r, :] = total[:, 2 * qw : 2 * qw + vw].astype(BF16)
        acc[r, 2 * qw + vw :] = total[:, 2 * qw + vw :]
        return carry

    lax.fori_loop(0, 4, finish, 0)
    poll(2)

    near_x = (mod(x + 2, nx), mod(x + 1, nx), mod(x - 1, nx), x)

    def retain(k):
        i = near_x[k]
        r = pl.ds(pl.multiple_of(i * quarter, quarter), quarter)
        seen = pl.ds(pl.multiple_of((nx - 1 - i) * quarter, quarter), seq)
        scores = lax.dot_general(
            qb[r, :], kb[...], (((1,), (1,)), ((), ())), preferred_element_type=F32
        )
        weighted = (scores * decay[:, seen]).astype(BF16)
        retained = jnp.dot(weighted, vb[...], preferred_element_type=F32)
        centred = retained - jnp.mean(retained, axis=-1, keepdims=True)
        normalized = centred * lax.rsqrt(
            jnp.mean(centred * centred, axis=-1, keepdims=True) + group_epsilon
        )
        gp[r, :] = (silu(acc[r, 2 * qw + vw :]) * normalized).astype(BF16)

    lo, hi = slice(0, half), slice(half, width)
    chunk = rows // 2

    def blocks_of(items):
        return [
            pl.ds(pl.multiple_of((2 * near_x[k] + cc) * rows + ch * chunk, chunk), chunk)
            for k, ch in items
            for cc in (0, 1)
        ]

    def load_rows(ref, items):
        return jnp.concatenate([ref[r, :] for r in blocks_of(items)], axis=0)

    class Reduce:
        def __init__(self, n, lhs, weight):
            self.n, self.lhs, self.weight = n, lhs, weight
            self.sends, self.got = [], {}

        def project(self, *items):
            n = self.n
            cols = width // 4

            def body(j, carry):
                at = pl.ds(pl.multiple_of(j * cols, cols), cols)
                product = jnp.dot(
                    load_rows(self.lhs, items), self.weight[:, at], preferred_element_type=F32
                ).astype(BF16)
                for i, r in enumerate(blocks_of(items)):
                    part[r, at] = product[i * chunk : (i + 1) * chunk]
                return carry

            lax.fori_loop(0, 4, body, 0)
            for k, ch in items:
                self.to_sibling(k, ch).start()

        def to_sibling(self, k, ch):
            start = pl.multiple_of((2 * near_x[k] + 1 - core) * rows + ch * chunk, chunk)
            return copy(
                part.at[pl.ds(start, chunk), :],
                sib_in.at[self.n, k, pl.ds(ch * chunk, chunk)],
                s_send.at[2 * k + ch],
                s_recv.at[2 * k + ch],
                sib,
            )

        def paired(self, k, ch):
            self.to_sibling(k, ch).wait_recv()

        def pre(self, k, ch, cols):
            at = pl.multiple_of((2 * near_x[k] + core) * rows + ch * chunk, chunk)
            r = slice(ch * chunk, (ch + 1) * chunk)
            return part[pl.ds(at, chunk), cols].astype(F32) + sib_in[self.n, k, r, cols].astype(F32)

        def ship(self, name, ch, slot_, value, cols, dst, device):
            n = self.n
            i = ch * 6 + ("pr", "pl", "dr", "dl", "sr", "sl").index(name)
            r = pl.ds(ch * chunk, chunk)
            stage[n, slot_, r, cols] = value.astype(BF16)
            s = copy(stage.at[n, slot_, r, cols], dst, r_send.at[i], r_recv.at[i], device)
            s.start()
            self.sends.append(s)
            self.got[name, ch] = s

        def passes(self, ch):
            self.paired(0, ch)
            n, r = self.n, pl.ds(ch * chunk, chunk)
            self.ship("pr", ch, 0, self.pre(0, ch, hi), hi, pass_in.at[n, 0, r], right)
            self.ship("pl", ch, 0, self.pre(0, ch, lo), lo, pass_in.at[n, 1, r], left)

        def direct_right(self, ch):
            self.paired(1, ch)
            dst = from_left.at[self.n, pl.ds(ch * chunk, chunk), lo]
            self.ship("dr", ch, 1, self.pre(1, ch, lo), lo, dst, right)

        def direct_left(self, ch):
            self.paired(2, ch)
            dst = from_right.at[self.n, pl.ds(ch * chunk, chunk), hi]
            self.ship("dl", ch, 2, self.pre(2, ch, hi), hi, dst, left)

        def sums(self, ch):
            n, r = self.n, pl.ds(ch * chunk, chunk)
            self.got["pr", ch].wait_recv()
            value = self.pre(1, ch, hi) + pass_in[n, 0, r].astype(F32)
            self.ship("sr", ch, 1, value, hi, from_left.at[n, r, hi], right)
            self.got["pl", ch].wait_recv()
            value = self.pre(2, ch, lo) + pass_in[n, 1, r].astype(F32)
            self.ship("sl", ch, 2, value, lo, from_right.at[n, r, lo], left)

        def arrive(self, ch):
            for name in ("dr", "dl", "sr", "sl"):
                self.got[name, ch].wait_recv()

        def total(self, at, count):
            n, r = self.n, pl.ds(at, count)
            base = pl.multiple_of((2 * x + core) * rows + at, count)
            return (
                (part[pl.ds(base, count), :].astype(F32) + sib_in[n, 3, r, :].astype(F32))
                + from_left[n, r, :].astype(F32)
                + from_right[n, r, :].astype(F32)
            )

        def drain(self):
            for s in self.sends:
                s.wait_send()
            for k in range(nx):
                self.to_sibling(k, 0).wait_send()
                self.to_sibling(k, 1).wait_send()

    one = Reduce(0, gp, w2)
    retain(0)
    y_whole(1)
    one.project((0, 0), (0, 1))
    poll()
    early = [polls.pop(0) for _ in range(4)]

    def neighbours():
        retain(1)
        pass_on(*early[0])
        one.project((1, 0), (1, 1))
        pass_on(*early[1])
        retain(2)
        pass_on(*early[2])
        one.project((2, 0), (2, 1))
        pass_on(*early[3])

    @pl.when(core == 1)
    def _():
        neighbours()

    one.passes(0)
    one.passes(1)

    @pl.when(core == 0)
    def _():
        neighbours()

    one.direct_right(0)
    poll()
    one.direct_left(0)
    retain(3)
    poll(2)
    one.sums(0)
    one.direct_right(1)
    one.direct_left(1)
    poll(2)
    one.project((3, 0), (3, 1))
    poll()
    one.sums(1)
    poll(3)
    one.paired(3, 0)
    one.paired(3, 1)
    poll(2)
    drain1()

    def mixed(i, carry):
        at = pl.multiple_of(i * 16, 16)
        after = tok[pl.ds(at, 16), :].astype(F32) + rms(one.total(at, 16)) * gains[1:2, :]
        am[pl.ds(at, 16), :] = after
        xw[pl.ds(pl.multiple_of(own + at, 16), 16), :] = (rms(after) * gains[2:3, :]).astype(BF16)
        return carry

    per = chunk // 16
    two = [gather(1, xw, 0, chunk), gather(2, xw, chunk, chunk)]
    one.arrive(0)
    lax.fori_loop(0, per, mixed, 0)
    two[0][0]()
    poll(4)
    one.arrive(1)
    lax.fori_loop(per, 2 * per, mixed, 0)
    two[1][0]()
    one.drain()
    poll(5)
    two[0][1]()
    poll(5)
    assert not polls

    def feed(*items):
        both = jnp.dot(load_rows(xw, items), w3[...], preferred_element_type=F32)
        hidden = (silu(both[:, 0:ff]) * both[:, ff:]).astype(BF16)
        for i, r in enumerate(blocks_of(items)):
            hid[r, :] = hidden[i * chunk : (i + 1) * chunk]

    last_one = Reduce(1, hid, w4)
    two[1][1]()
    y_whole(2)
    two[0][4]()
    feed((1, 0), (2, 0))
    y_whole(3)
    last_one.project((1, 0), (2, 0))
    two[0][2]()
    two[1][4]()
    feed((1, 1), (2, 1))
    last_one.direct_right(0)
    last_one.direct_left(0)
    last_one.project((1, 1), (2, 1))
    two[1][2]()
    two[0][5]()
    feed((0, 0))
    last_one.project((0, 0))
    last_one.direct_right(1)
    last_one.direct_left(1)
    two[1][5]()
    feed((0, 1))
    last_one.passes(0)
    last_one.project((0, 1))
    two[0][3]()
    two[1][3]()
    feed((3, 0), (3, 1))
    last_one.passes(1)
    last_one.project((3, 0), (3, 1))
    last_one.sums(0)
    last_one.sums(1)
    last_one.paired(3, 0)
    last_one.paired(3, 1)

    def last(i, carry):
        at = pl.multiple_of(i * 16, 16)
        r = pl.ds(at, 16)
        out[r, :] = (am[r, :] + rms(last_one.total(at, 16)) * gains[3:4, :]).astype(BF16)
        return carry

    last_one.arrive(0)
    lax.fori_loop(0, per, last, 0)
    last_one.arrive(1)
    lax.fori_loop(per, 2 * per, last, 0)
    two[0][6]()
    two[1][6]()
    last_one.drain()
    for a in range(4):
        y_drain(a)


def layer(nf, nx, tokens, gains, wq, wk, wv, ws, wo, wg, wu, wd):
    rows, width = tokens.shape
    seq = rows * 2 * nx
    qw, vw, ff = wq.shape[1], wv.shape[1], wg.shape[1]
    frequency = 10000.0 ** (-np.linspace(0.0, 1.0, qw // 2))
    within = np.arange(seq // 4, dtype=np.float64)[:, None] * frequency[None, :]
    starts = np.arange(4, dtype=np.float64)[:, None] * (seq // 4) * frequency[None, :]
    turn = jnp.asarray(np.stack([np.cos(within), np.sin(within)]).astype(np.float32))
    base = jnp.asarray(np.concatenate([np.cos(starts), np.sin(starts)]).astype(np.float32))
    heads = np.arange(2 * nx, dtype=np.float64)
    lam = -(4.0 / BLOCK) * (BLOCK / (32.0 * seq)) ** (heads / (H - 1))
    lam = jnp.asarray(np.repeat(lam[:, None], 128, axis=1).astype(np.float32))
    vmem = pl.BlockSpec(memory_space=pltpu.VMEM)
    hbm = pl.BlockSpec(memory_space=pl.ANY)
    dma = pltpu.SemaphoreType.DMA
    far = nf // 2
    half = width // 2
    n1 = 2 * qw + 2 * vw
    return pl.pallas_call(
        functools.partial(kernel, nf, nx),
        out_shape=jax.ShapeDtypeStruct((rows, width), BF16),
        in_specs=[hbm] * 13,
        out_specs=vmem,
        scratch_shapes=[
            pltpu.VMEM((width, n1), BF16),
            pltpu.VMEM((wo.shape[0], width), BF16),
            pltpu.VMEM((width, 2 * ff), BF16),
            pltpu.VMEM((wd.shape[0], width), BF16),
            pltpu.VMEM((seq, width), BF16),
            pltpu.VMEM((seq, width), BF16),
            pltpu.VMEM((seq, n1), F32),
            pltpu.VMEM((seq, qw), BF16),
            pltpu.VMEM((seq, qw), BF16),
            pltpu.VMEM((seq, vw), BF16),
            pltpu.VMEM((seq, vw), BF16),
            pltpu.VMEM((seq, ff), BF16),
            pltpu.VMEM((seq, width), BF16),
            pltpu.VMEM((2, nx, rows, width), BF16),
            pltpu.VMEM((2, 3, rows, width), BF16),
            pltpu.VMEM((2, 2, rows, half), BF16),
            pltpu.VMEM((2, rows, width), BF16),
            pltpu.VMEM((2, rows, width), BF16),
            pltpu.VMEM((rows, width), F32),
            pltpu.VMEM((2, seq // 4, qw // 2), F32),
            pltpu.VMEM((seq // 4, 2 * seq - seq // 4), F32),
            pltpu.VMEM(tokens.shape, BF16),
            pltpu.VMEM(gains.shape, F32),
            pltpu.VMEM(lam.shape, F32),
            pltpu.VMEM(base.shape, F32),
            dma((13,)),
            dma((24,)),
            dma((12, far)),
            dma((12,)),
            dma((2 * far + 3,)),
            dma((2, 9)),
            dma((2, 9)),
            dma((8,)),
            dma((8,)),
            dma((12,)),
            dma((12,)),
        ],
        compiler_params=pltpu.CompilerParams(
            collective_id=0, has_side_effects=True, vmem_limit_bytes=66_000_000
        ),
    )(tokens, gains, lam, turn, base, wq, wk, wv, ws, wo, wg, wu, wd)


def solution(mesh):
    placed = (
        P(("grp", "fs", "tp"), None),
        P(),
        P("fs", "tp"),
        P("fs", "tp"),
        P("fs", "tp"),
        P("fs", "tp"),
        P("tp", "fs"),
        P("fs", "tp"),
        P("fs", "tp"),
        P("tp", "fs"),
    )
    nf, nt = mesh.shape["fs"], mesh.shape["tp"]
    assert mesh.shape["grp"] % 2 == 0 and nt == 8 and nf % 2 == 0
    return jax.shard_map(
        functools.partial(layer, nf, nt // 2),
        mesh=mesh,
        in_specs=placed,
        out_specs=P(("grp", "fs", "tp"), None),
        check_vma=False,
    )
```

```python
import functools

import jax
import jax.numpy as jnp
import numpy as np
from jax import lax
from jax.experimental import pallas as pl
from jax.experimental.pallas import tpu as pltpu
from jax.sharding import PartitionSpec as P

H = 8
BLOCK = 128
norm_epsilon = 1e-06
group_epsilon = 0.01
MESH = pl.DeviceIdType.MESH
F32 = jnp.float32
BF16 = jnp.bfloat16


def mod(a, n):
    return lax.rem(a + n, n)


def rms(matrix):
    return matrix * lax.rsqrt(jnp.mean(matrix * matrix, axis=-1, keepdims=True) + norm_epsilon)


def silu(v):
    return v / (1.0 + jnp.exp(-v))


def kernel(
    nf,
    nx,
    tok_hbm,
    gains_hbm,
    lam_hbm,
    turn_hbm,
    base_hbm,
    wq,
    wk,
    wv,
    ws,
    wo,
    wg,
    wu,
    wd,
    out_hbm,
    w1,
    w2,
    w3,
    w4,
    xn,
    xw,
    acc,
    qb,
    kb,
    vb,
    gp,
    hid,
    part,
    sib_in,
    stage,
    pass_in,
    from_left,
    from_right,
    am,
    turn,
    decay,
    tok,
    gains,
    lam_ref,
    base_ref,
    out,
    local_sem,
    z_send,
    z_recv,
    y_send,
    y_recv,
    g_send,
    g_recv,
    s_send,
    s_recv,
    r_send,
    r_recv,
):
    rows, width = tok.shape
    seq = xn.shape[0]
    half = width // 2
    quarter = seq // 4
    me = lax.axis_index("fs")
    tp = lax.axis_index("tp")
    group = lax.axis_index("grp")
    x = tp // 2
    core = lax.rem(tp, 2)
    plane = lax.rem(group, 2)
    up = {"fs": mod(me + 1, nf)}
    down = {"fs": mod(me - 1, nf)}
    pair = {"grp": group + 1 - 2 * plane}
    sib = {"tp": 2 * x + 1 - core}
    right = {"tp": 2 * mod(x + 1, nx) + core}
    left = {"tp": 2 * mod(x - 1, nx) + core}

    def copy(src, dst, send, recv, device):
        return pltpu.make_async_remote_copy(
            src_ref=src,
            dst_ref=dst,
            send_sem=send,
            recv_sem=recv,
            device_id=device,
            device_id_type=MESH,
        )

    kd = wq.shape[0]
    mine = pl.ds(pl.multiple_of(me * kd, kd), kd)
    mine_cols = pl.ds(pl.multiple_of(me * kd, kd), kd)
    qw, vw, ff = wq.shape[1], wv.shape[1], wg.shape[1]
    locals_ = [
        (wq, w1.at[mine, 0:qw]),
        (wk, w1.at[mine, qw : 2 * qw]),
        (wv, w1.at[mine, 2 * qw : 2 * qw + vw]),
        (ws, w1.at[mine, 2 * qw + vw : 2 * qw + 2 * vw]),
        (wo, w2.at[:, mine_cols]),
        (wg, w3.at[mine, 0:ff]),
        (wu, w3.at[mine, ff : 2 * ff]),
        (wd, w4.at[:, mine_cols]),
        (turn_hbm, turn),
        (lam_hbm, lam_ref),
        (base_hbm, base_ref),
        (tok_hbm, tok),
        (gains_hbm, gains),
    ]
    loads = [
        pltpu.make_async_copy(src, dst, local_sem.at[i]) for i, (src, dst) in enumerate(locals_)
    ]
    for load in loads[-2:] + loads[:-2]:
        load.start()

    barrier = pltpu.get_barrier_semaphore()
    for device in (up, down, pair, sib, right, left):
        pl.semaphore_signal(barrier, inc=1, device_id=device, device_id_type=MESH)

    own = pl.multiple_of(tp * rows, rows)

    def norm_in(i, carry):
        at = pl.multiple_of(i * 16, 16)
        value = rms(tok[pl.ds(at, 16), :].astype(F32)) * gains[0:1, :]
        xn[pl.ds(own + at, 16), :] = value.astype(BF16)
        return carry

    for load in loads[-2:]:
        load.wait()
    lax.fori_loop(0, rows // 16, norm_in, 0)
    pl.semaphore_wait(barrier, 6)

    def shared(a):
        return w2.shape[0] // 4 if a == 1 else w4.shape[0] // 3

    pieces = (4, 2, 4, 2)
    owns = (2, 1, 2, 1)

    def place(a, owner, piece, plane_, rows_half=None):
        ref = (w1, w2, w3, w4)[a]
        if a in (0, 2):
            w = ref.shape[1] // 3 // owns[a]
            start, count = owner * kd, kd
            if rows_half is not None:
                count = kd // 2
                start = start + rows_half * count
            r = pl.ds(pl.multiple_of(start, kd // 2), count)
            if piece < owns[a]:
                at = pl.multiple_of(plane_ * 2 * w * owns[a] + piece * w, 128)
            else:
                at = piece * w
            return ref.at[r, pl.ds(at, w)]
        t = shared(a)
        mid = ref.shape[0] - 2 * t
        r = pl.ds(pl.multiple_of(plane_ * (t + mid), 16), t) if piece == 0 else pl.ds(t, mid)
        return ref.at[r, pl.ds(pl.multiple_of(owner * kd, kd), kd)]

    half_streams = 2 * (pieces[0] + pieces[1])

    def z_index(a, d, piece):
        return 2 * sum(pieces[:a]) + d * pieces[a] + piece

    def y_index(a, d, piece):
        return 2 * sum(owns[:a]) + d * owns[a] + piece

    def owner_of(d, s):
        return mod(me - s, nf) if d == 0 else lax.rem(me + s, nf)

    far = nf // 2

    def z_copy(a, d, piece, s, rows_half=None):
        src = place(a, owner_of(d, s - 1), piece, plane, rows_half)
        k = z_index(a, d, piece)
        return copy(src, src, z_send.at[k], z_recv.at[k % half_streams, s - 1], up if d == 0 else down)

    def z_arrived(a, d, piece, s, rows_half=None):
        dst = place(a, owner_of(d, s), piece, plane, rows_half)
        k = z_index(a, d, piece)
        copy(dst, dst, z_send.at[k], z_recv.at[k % half_streams, s - 1], up if d == 0 else down).wait_recv()

    def y_sem(a, d, s):
        return y_recv.at[d * far + s - 1] if a == 0 else y_recv.at[2 * far + a - 1]

    def y_copy(a, d, piece, s, rows_half=None):
        src = place(a, owner_of(d, s), piece, plane, rows_half)
        return copy(src, src, y_send.at[y_index(a, d, piece)], y_sem(a, d, s), pair)

    def last_half(a, d):
        return d if a in (0, 2) else None

    def has_last(a, d):
        return a in (0, 2) or (a == 1 and d == 0) or (a == 3 and d == 1)

    def begin(a):
        for piece in range(pieces[a]):
            for d in (0, 1):
                z_copy(a, d, piece, 1).start()

    def forward(a, s, piece):
        for d in (0, 1):
            here = s < far or has_last(a, d)
            part_of = last_half(a, d) if s == far else None
            if here:
                z_arrived(a, d, piece, s, part_of)
                z_copy(a, d, piece, s, part_of).wait_send()
            if s < far - 1:
                z_copy(a, d, piece, s + 1).start()
            elif s == far - 1 and has_last(a, d):
                z_copy(a, d, piece, far, last_half(a, d)).start()
            if piece < owns[a]:
                if s > 1:
                    y_copy(a, d, piece, s - 1).wait_send()
                if here:
                    y_copy(a, d, piece, s, part_of).start()

    def slot(*items):
        for piece in range(4):
            for a, s in items:
                if piece < pieces[a]:
                    forward(a, s, piece)

    def y_step(s):
        w = w1.shape[1] // 3
        for d in (0, 1):
            count = kd if s < far else kd // 2
            start = owner_of(d, s) * kd + (0 if s < far else d * count)
            at = pl.multiple_of((1 - plane) * 2 * w, 128)
            dst = w1.at[pl.ds(pl.multiple_of(start, kd // 2), count), pl.ds(at, w)]
            copy(dst, dst, y_send.at[0], y_sem(0, d, s), pair).wait_recv()

    def y_whole(a):
        ref = (w1, w2, w3, w4)[a]
        n = (nf - 1) * kd
        if a == 2:
            w = ref.shape[1] // 3
            dst = ref.at[0:n, pl.ds(pl.multiple_of((1 - plane) * 2 * w, 128), w)]
        else:
            t = shared(a)
            dst = ref.at[pl.ds(pl.multiple_of((1 - plane) * (ref.shape[0] - t), 16), t), 0:n]
        copy(dst, dst, y_send.at[0], y_sem(a, 0, 1), pair).wait_recv()

    def y_drain(a):
        for piece in range(owns[a]):
            for d in (0, 1):
                if has_last(a, d):
                    y_copy(a, d, piece, far, last_half(a, d)).wait_send()

    def gather(n, ref, at, count):
        at_left, at_right, at_far = mod(x - 1, nx), mod(x + 1, nx), mod(x + 2, nx)
        lo, hi = pl.ds(0, half), pl.ds(half, half)
        every = pl.ds(0, width)

        def whole(xx, cc, cols=every):
            return ref.at[pl.ds(pl.multiple_of((2 * xx + cc) * rows + at, count), count), cols]

        def send(k, xx, cols, device):
            src = whole(xx, core, cols)
            return copy(src, src, g_send.at[n // 2, k], g_recv.at[n // 2, k], device)

        def arrived(k, xx, cc, cols):
            dst = whole(xx, cc, cols)
            copy(dst, dst, g_send.at[n // 2, k], g_recv.at[n // 2, k], sib).wait_recv()

        sends = []

        def go(*args):
            s = send(*args)
            s.start()
            sends.append(s)

        def first():
            go(1, x, every, right)
            go(2, x, every, left)
            go(0, x, every, sib)

        def second():
            arrived(1, at_left, core, every)
            go(3, at_left, lo, right)
            go(4, at_left, every, sib)
            arrived(2, at_right, core, every)
            go(5, at_right, hi, left)
            go(6, at_right, every, sib)

        def third_():
            arrived(3, at_far, core, lo)
            go(7, at_far, lo, sib)
            arrived(5, at_far, core, hi)
            go(8, at_far, hi, sib)

        def own_chip():
            arrived(0, x, 1 - core, every)

        def near():
            arrived(4, at_left, 1 - core, every)
            arrived(6, at_right, 1 - core, every)

        def rest():
            arrived(7, at_far, 1 - core, lo)
            arrived(8, at_far, 1 - core, hi)

        def drain():
            for s in sends:
                s.wait_send()

        return first, second, third_, own_chip, near, rest, drain

    for load in loads[:4]:
        load.wait()
    begin(0)
    first, second, third_, own_chip, near, rest, drain1 = gather(0, xn, 0, rows)
    first()

    for load in loads[4:-2]:
        load.wait()

    lam = lam_ref[pl.ds(tp, 1), 0:1]
    dn = lax.broadcasted_iota(jnp.int32, decay.shape, 0) + (seq - quarter)
    dm = lax.broadcasted_iota(jnp.int32, decay.shape, 1)
    dist = (dn - dm).astype(F32)
    decay[...] = jnp.where(dist >= 0.0, jnp.exp(lam * jnp.maximum(dist, 0.0)), 0.0)

    def k_slice(owner):
        return pl.ds(pl.multiple_of(owner * kd, kd), kd)

    def tiled(tiles, body):
        n = acc.shape[1] // 2

        def step(i, carry):
            r = pl.ds(pl.multiple_of(i // 2 * quarter, quarter), quarter)
            body(r, pl.ds(pl.multiple_of(lax.rem(i, 2) * n, n), n))
            return carry

        lax.fori_loop(2 * tiles[0], 2 * tiles[1], step, 0)

    def add_own(tiles):
        def body(r, c):
            acc[r, c] = jnp.dot(
                xn[r, k_slice(me)], w1[k_slice(me), c], preferred_element_type=F32
            )

        tiled(tiles, body)

    def add_two(s, tiles):
        a, b = k_slice(owner_of(0, s)), k_slice(owner_of(1, s))

        def body(r, c):
            acc[r, c] = (
                acc[r, c]
                + jnp.dot(xn[r, a], w1[a, c], preferred_element_type=F32)
                + jnp.dot(xn[r, b], w1[b, c], preferred_element_type=F32)
            )

        tiled(tiles, body)

    def slot_and_add(s, adds):
        for piece in range(4):
            forward(0, s, piece)
            if piece < 3:
                for waits, add, tiles in adds[piece]:
                    if waits:
                        y_step(waits)
                    add(tiles)
        forward(1, s, 0)
        forward(1, s, 1)

    order = (((2, 0), (3, 0)), ((2, 1),), ((2, 2), (3, 1)), ((2, 3),))
    polls = [(s, group) for s in range(1, far + 1) for group in order]

    def pass_on(s, group):
        for a, piece in group:
            forward(a, s, piece)

    def poll(count=1):
        for _ in range(count):
            pass_on(*polls.pop(0))

    def begin_polled():
        for group in order:
            for a, piece in group:
                for d in (0, 1):
                    z_copy(a, d, piece, 1).start()

    def two_of(s, tiles, wait=True):
        return s if wait else 0, functools.partial(add_two, s), tiles

    begin(1)
    slot((0, 1))
    forward(1, 1, 0)
    forward(1, 1, 1)
    second()
    slot((0, 2))
    forward(1, 2, 0)
    forward(1, 2, 1)
    own_chip()
    third_()
    forward(0, 3, 0)
    forward(0, 3, 1)
    near()
    rest()
    forward(0, 3, 2)
    forward(0, 3, 3)
    forward(1, 3, 0)
    forward(1, 3, 1)
    slot_and_add(4, ([(0, add_own, (0, 4))], [two_of(1, (0, 4))], [two_of(2, (0, 4))]))
    slot_and_add(5, ([two_of(3, (0, 4))], [], [two_of(4, (0, 4))]))
    for s in range(6, far):
        slot_and_add(s, ([], [], [two_of(s - 1, (0, 4))]))
    begin_polled()
    slot_and_add(far, ([], [two_of(far - 1, (0, 2))], [two_of(far - 1, (2, 4), False)]))
    y_step(far)
    far_slice = k_slice(owner_of(0, far))

    key_scale = float(qw) ** -0.5
    hq = qw // 2

    def finish(i, carry):
        r = pl.ds(pl.multiple_of(i * quarter, quarter), quarter)
        total = acc[r, :] + jnp.dot(xn[r, far_slice], w1[far_slice, :], preferred_element_type=F32)
        cb, sb = base_ref[pl.ds(i, 1), :], base_ref[pl.ds(i + 4, 1), :]
        c = cb * turn[0] - sb * turn[1]
        s = sb * turn[0] + cb * turn[1]
        for ref, at, scale in ((qb, 0, None), (kb, qw, key_scale)):
            a, b = total[:, at : at + hq], total[:, at + hq : at + qw]
            first_half = a * c - b * s
            second_half = a * s + b * c
            if scale is not None:
                first_half, second_half = first_half * scale, second_half * scale
            ref[r, 0:hq] = first_half.astype(BF16)
            ref[r, hq:qw] = second_half.astype(BF16)
        vb[r, :] = total[:, 2 * qw : 2 * qw + vw].astype(BF16)
        acc[r, 2 * qw + vw :] = total[:, 2 * qw + vw :]
        return carry

    lax.fori_loop(0, 4, finish, 0)
    poll(2)

    near_x = (mod(x + 2, nx), mod(x + 1, nx), mod(x - 1, nx), x)

    def retain(k):
        i = near_x[k]
        r = pl.ds(pl.multiple_of(i * quarter, quarter), quarter)
        seen = pl.ds(pl.multiple_of((nx - 1 - i) * quarter, quarter), seq)
        scores = lax.dot_general(
            qb[r, :], kb[...], (((1,), (1,)), ((), ())), preferred_element_type=F32
        )
        weighted = (scores * decay[:, seen]).astype(BF16)
        retained = jnp.dot(weighted, vb[...], preferred_element_type=F32)
        centred = retained - jnp.mean(retained, axis=-1, keepdims=True)
        normalized = centred * lax.rsqrt(
            jnp.mean(centred * centred, axis=-1, keepdims=True) + group_epsilon
        )
        gp[r, :] = (silu(acc[r, 2 * qw + vw :]) * normalized).astype(BF16)

    lo, hi = slice(0, half), slice(half, width)
    chunk = rows // 2

    def blocks_of(items):
        return [
            pl.ds(pl.multiple_of((2 * near_x[k] + cc) * rows + ch * chunk, chunk), chunk)
            for k, ch in items
            for cc in (0, 1)
        ]

    def load_rows(ref, items):
        return jnp.concatenate([ref[r, :] for r in blocks_of(items)], axis=0)

    class Reduce:
        def __init__(self, n, lhs, weight):
            self.n, self.lhs, self.weight = n, lhs, weight
            self.sends, self.got = [], {}

        def project(self, *items):
            n = self.n
            cols = width // 4

            def body(j, carry):
                at = pl.ds(pl.multiple_of(j * cols, cols), cols)
                product = jnp.dot(
                    load_rows(self.lhs, items), self.weight[:, at], preferred_element_type=F32
                ).astype(BF16)
                for i, r in enumerate(blocks_of(items)):
                    part[r, at] = product[i * chunk : (i + 1) * chunk]
                return carry

            lax.fori_loop(0, 4, body, 0)
            for k, ch in items:
                self.to_sibling(k, ch).start()

        def to_sibling(self, k, ch):
            start = pl.multiple_of((2 * near_x[k] + 1 - core) * rows + ch * chunk, chunk)
            return copy(
                part.at[pl.ds(start, chunk), :],
                sib_in.at[self.n, k, pl.ds(ch * chunk, chunk)],
                s_send.at[2 * k + ch],
                s_recv.at[2 * k + ch],
                sib,
            )

        def paired(self, k, ch):
            self.to_sibling(k, ch).wait_recv()

        def pre(self, k, ch, cols):
            at = pl.multiple_of((2 * near_x[k] + core) * rows + ch * chunk, chunk)
            r = slice(ch * chunk, (ch + 1) * chunk)
            return part[pl.ds(at, chunk), cols].astype(F32) + sib_in[self.n, k, r, cols].astype(F32)

        def ship(self, name, ch, slot_, value, cols, dst, device):
            n = self.n
            i = ch * 6 + ("pr", "pl", "dr", "dl", "sr", "sl").index(name)
            r = pl.ds(ch * chunk, chunk)
            stage[n, slot_, r, cols] = value.astype(BF16)
            s = copy(stage.at[n, slot_, r, cols], dst, r_send.at[i], r_recv.at[i], device)
            s.start()
            self.sends.append(s)
            self.got[name, ch] = s

        def passes(self, ch):
            self.paired(0, ch)
            n, r = self.n, pl.ds(ch * chunk, chunk)
            self.ship("pr", ch, 0, self.pre(0, ch, hi), hi, pass_in.at[n, 0, r], right)
            self.ship("pl", ch, 0, self.pre(0, ch, lo), lo, pass_in.at[n, 1, r], left)

        def direct_right(self, ch):
            self.paired(1, ch)
            dst = from_left.at[self.n, pl.ds(ch * chunk, chunk), lo]
            self.ship("dr", ch, 1, self.pre(1, ch, lo), lo, dst, right)

        def direct_left(self, ch):
            self.paired(2, ch)
            dst = from_right.at[self.n, pl.ds(ch * chunk, chunk), hi]
            self.ship("dl", ch, 2, self.pre(2, ch, hi), hi, dst, left)

        def sums(self, ch):
            n, r = self.n, pl.ds(ch * chunk, chunk)
            self.got["pr", ch].wait_recv()
            value = self.pre(1, ch, hi) + pass_in[n, 0, r].astype(F32)
            self.ship("sr", ch, 1, value, hi, from_left.at[n, r, hi], right)
            self.got["pl", ch].wait_recv()
            value = self.pre(2, ch, lo) + pass_in[n, 1, r].astype(F32)
            self.ship("sl", ch, 2, value, lo, from_right.at[n, r, lo], left)

        def arrive(self, ch):
            for name in ("dr", "dl", "sr", "sl"):
                self.got[name, ch].wait_recv()

        def total(self, at, count):
            n, r = self.n, pl.ds(at, count)
            base = pl.multiple_of((2 * x + core) * rows + at, count)
            return (
                (part[pl.ds(base, count), :].astype(F32) + sib_in[n, 3, r, :].astype(F32))
                + from_left[n, r, :].astype(F32)
                + from_right[n, r, :].astype(F32)
            )

        def drain(self):
            for s in self.sends:
                s.wait_send()
            for k in range(nx):
                self.to_sibling(k, 0).wait_send()
                self.to_sibling(k, 1).wait_send()

    one = Reduce(0, gp, w2)
    retain(0)
    y_whole(1)
    one.project((0, 0), (0, 1))
    poll()
    early = [polls.pop(0) for _ in range(4)]

    def neighbours():
        retain(1)
        pass_on(*early[0])
        one.project((1, 0), (1, 1))
        pass_on(*early[1])
        retain(2)
        pass_on(*early[2])
        one.project((2, 0), (2, 1))
        pass_on(*early[3])

    @pl.when(core == 1)
    def _():
        neighbours()

    one.passes(0)
    one.passes(1)

    @pl.when(core == 0)
    def _():
        neighbours()

    one.direct_right(0)
    poll()
    one.direct_left(0)
    retain(3)
    poll(2)
    one.sums(0)
    one.direct_right(1)
    one.direct_left(1)
    poll(2)
    one.project((3, 0), (3, 1))
    poll()
    one.sums(1)
    poll(3)
    one.paired(3, 0)
    one.paired(3, 1)
    poll(2)
    drain1()

    def mixed(i, carry):
        at = pl.multiple_of(i * 16, 16)
        after = tok[pl.ds(at, 16), :].astype(F32) + rms(one.total(at, 16)) * gains[1:2, :]
        am[pl.ds(at, 16), :] = after
        xw[pl.ds(pl.multiple_of(own + at, 16), 16), :] = (rms(after) * gains[2:3, :]).astype(BF16)
        return carry

    per = chunk // 16
    two = [gather(1, xw, 0, chunk), gather(2, xw, chunk, chunk)]
    one.arrive(0)
    lax.fori_loop(0, per, mixed, 0)
    two[0][0]()
    poll(4)
    one.arrive(1)
    lax.fori_loop(per, 2 * per, mixed, 0)
    two[1][0]()
    one.drain()
    poll(5)
    two[0][1]()
    poll(5)
    assert not polls

    def feed(*items):
        both = jnp.dot(load_rows(xw, items), w3[...], preferred_element_type=F32)
        hidden = (silu(both[:, 0:ff]) * both[:, ff:]).astype(BF16)
        for i, r in enumerate(blocks_of(items)):
            hid[r, :] = hidden[i * chunk : (i + 1) * chunk]

    last_one = Reduce(1, hid, w4)
    two[1][1]()
    y_whole(2)
    two[0][4]()
    feed((1, 0), (2, 0))
    y_whole(3)
    last_one.project((1, 0), (2, 0))
    two[0][2]()
    two[1][4]()
    feed((1, 1), (2, 1))
    last_one.direct_right(0)
    last_one.direct_left(0)
    last_one.project((1, 1), (2, 1))
    two[1][2]()
    two[0][5]()
    feed((0, 0))
    last_one.project((0, 0))
    last_one.direct_right(1)
    last_one.direct_left(1)
    two[1][5]()
    feed((0, 1))
    last_one.passes(0)
    last_one.project((0, 1))
    two[0][3]()
    two[1][3]()
    feed((3, 0), (3, 1))
    last_one.passes(1)
    last_one.project((3, 0), (3, 1))
    last_one.sums(0)
    last_one.sums(1)
    last_one.paired(3, 0)
    last_one.paired(3, 1)

    def last(i, carry):
        at = pl.multiple_of(i * 16, 16)
        r = pl.ds(at, 16)
        out[r, :] = (am[r, :] + rms(last_one.total(at, 16)) * gains[3:4, :]).astype(BF16)
        return carry

    last_one.arrive(0)
    lax.fori_loop(0, per, last, 0)
    leave = [
        pltpu.make_async_copy(
            out.at[pl.ds(ch * chunk, chunk)], out_hbm.at[pl.ds(ch * chunk, chunk)], local_sem.at[ch]
        )
        for ch in (0, 1)
    ]
    leave[0].start()
    last_one.arrive(1)
    lax.fori_loop(per, 2 * per, last, 0)
    leave[1].start()
    leave[0].wait()
    leave[1].wait()
    two[0][6]()
    two[1][6]()
    last_one.drain()
    for a in range(4):
        y_drain(a)


def layer(nf, nx, tokens, gains, wq, wk, wv, ws, wo, wg, wu, wd):
    rows, width = tokens.shape
    seq = rows * 2 * nx
    qw, vw, ff = wq.shape[1], wv.shape[1], wg.shape[1]
    frequency = 10000.0 ** (-np.linspace(0.0, 1.0, qw // 2))
    within = np.arange(seq // 4, dtype=np.float64)[:, None] * frequency[None, :]
    starts = np.arange(4, dtype=np.float64)[:, None] * (seq // 4) * frequency[None, :]
    turn = jnp.asarray(np.stack([np.cos(within), np.sin(within)]).astype(np.float32))
    base = jnp.asarray(np.concatenate([np.cos(starts), np.sin(starts)]).astype(np.float32))
    heads = np.arange(2 * nx, dtype=np.float64)
    lam = -(4.0 / BLOCK) * (BLOCK / (32.0 * seq)) ** (heads / (H - 1))
    lam = jnp.asarray(np.repeat(lam[:, None], 128, axis=1).astype(np.float32))
    hbm = pl.BlockSpec(memory_space=pl.ANY)
    dma = pltpu.SemaphoreType.DMA
    far = nf // 2
    half = width // 2
    n1 = 2 * qw + 2 * vw
    return pl.pallas_call(
        functools.partial(kernel, nf, nx),
        out_shape=jax.ShapeDtypeStruct((rows, width), BF16),
        in_specs=[hbm] * 13,
        out_specs=hbm,
        scratch_shapes=[
            pltpu.VMEM((width, n1), BF16),
            pltpu.VMEM((wo.shape[0], width), BF16),
            pltpu.VMEM((width, 2 * ff), BF16),
            pltpu.VMEM((wd.shape[0], width), BF16),
            pltpu.VMEM((seq, width), BF16),
            pltpu.VMEM((seq, width), BF16),
            pltpu.VMEM((seq, n1), F32),
            pltpu.VMEM((seq, qw), BF16),
            pltpu.VMEM((seq, qw), BF16),
            pltpu.VMEM((seq, vw), BF16),
            pltpu.VMEM((seq, vw), BF16),
            pltpu.VMEM((seq, ff), BF16),
            pltpu.VMEM((seq, width), BF16),
            pltpu.VMEM((2, nx, rows, width), BF16),
            pltpu.VMEM((2, 3, rows, width), BF16),
            pltpu.VMEM((2, 2, rows, half), BF16),
            pltpu.VMEM((2, rows, width), BF16),
            pltpu.VMEM((2, rows, width), BF16),
            pltpu.VMEM((rows, width), F32),
            pltpu.VMEM((2, seq // 4, qw // 2), F32),
            pltpu.VMEM((seq // 4, 2 * seq - seq // 4), F32),
            pltpu.VMEM(tokens.shape, BF16),
            pltpu.VMEM(gains.shape, F32),
            pltpu.VMEM(lam.shape, F32),
            pltpu.VMEM(base.shape, F32),
            pltpu.VMEM((rows, width), BF16),
            dma((13,)),
            dma((24,)),
            dma((12, far)),
            dma((12,)),
            dma((2 * far + 3,)),
            dma((2, 9)),
            dma((2, 9)),
            dma((8,)),
            dma((8,)),
            dma((12,)),
            dma((12,)),
        ],
        compiler_params=pltpu.CompilerParams(
            collective_id=0, has_side_effects=True, vmem_limit_bytes=66_000_000
        ),
    )(tokens, gains, lam, turn, base, wq, wk, wv, ws, wo, wg, wu, wd)


def solution(mesh):
    placed = (
        P(("grp", "fs", "tp"), None),
        P(),
        P("fs", "tp"),
        P("fs", "tp"),
        P("fs", "tp"),
        P("fs", "tp"),
        P("tp", "fs"),
        P("fs", "tp"),
        P("fs", "tp"),
        P("tp", "fs"),
    )
    nf, nt = mesh.shape["fs"], mesh.shape["tp"]
    assert mesh.shape["grp"] % 2 == 0 and nt == 8 and nf % 2 == 0
    return jax.shard_map(
        functools.partial(layer, nf, nt // 2),
        mesh=mesh,
        in_specs=placed,
        out_specs=P(("grp", "fs", "tp"), None),
        check_vma=False,
    )
```
